512 devices in a mesh: grp: 2 (over y), sp: 16 (over z), dp: 16 (over x, core).
Axes of the slice: x: 8, y: 2, z: 16, core: 2. Of those that a mesh axis runs over, the one named last changes fastest.
The devices are a block of a 8x8x16 slice.
Arguments:
- tokens: bfloat16 [32, 2048, 2048], P(('grp', 'dp'), 'sp'), parts along dimension 0, may hold values from -6 to 6
- forget_offset: float32 [32, 2048], P(('grp', 'dp'), 'sp'), parts along dimension 0, may hold values from -1.2 to 1.2, as said below
- q_weight: bfloat16 [2048, 2048], P(None, 'dp'), may hold values from -0.125 to 0.125
- k_weight: bfloat16 [2048, 512], P(None, 'dp'), may hold values from -0.125 to 0.125
- v_weight: bfloat16 [2048, 512], P(None, 'dp'), may hold values from -0.125 to 0.125
- forget_weight: bfloat16 [2048, 16], replicated, may hold values from -0.125 to 0.125
- forget_bias: float32 [16], replicated, may hold values from 3 to 12
- score_gain: float32 [16], replicated, may hold values from 0.5 to 80
- out_gain: float32 [2048], replicated, may hold values from 0.1 to 1.9
Outputs:
- attended: bfloat16 [32, 2048, 2048], P(('grp', 'dp'), 'sp'), parts along dimension 0
The draws below stay inside these ranges and needn't reach their ends.
There are 2 independent parts, one for each index of `grp`. The reference program is written for one: setup_inputs(seed, part) draws one part's arguments, and reference() takes and returns one part's arrays. A program takes and returns all parts, laid end to end along the dimension named above; an argument that names none is the same for every part. Nothing has to cross between parts.
Inputs may be any that keep to these rules, and one draw needn't show every extreme that they name: `forget_offset`: constant over aligned spans of 64 positions.
All inputs are finite; a program needn't handle non-finite values.
Results may differ from the reference program's by a relative error of at most 0.0085.
The reference program's roundings to bfloat16 on the way count: a program that leaves them out, or rounds other values in their place, can miss the bound.
Values may be sent and summed in bfloat16 or wider, within the bound.
No kernel may reach another device: no remote copies, remote signals or barrier semaphores. Data moves between devices by JAX's collectives and lax.ppermute only.
A program may use at most 128 MiB of HBM per device.

```python
import jax
import jax.numpy as jnp
from jax import lax

WIDTH = 2048
HEADS = 16
KV_HEADS = 4
HEAD_DIM = 128
SEQ_LEN = 2048
SEQS = 16


def draw_forget_offset(key, part):
    spans = (SEQ_LEN + 63) // 64
    levels = jax.random.uniform(key, (SEQS, spans), jnp.float32, -1.2, 1.2)
    return jnp.repeat(levels, 64, axis=1)[:, :SEQ_LEN]


def draw_forget_bias(key, part):
    head_order = jax.random.permutation(jax.random.fold_in(key, 11), HEADS)
    jitter = jax.random.uniform(jax.random.fold_in(key, 12), (HEADS,), jnp.float32, -0.3, 0.3)
    slow_level = jnp.log(2.0 * SEQ_LEN)
    fast_level = jnp.log(40.0)
    return jnp.where(head_order < HEADS // 2, slow_level, fast_level) + jitter


def draw_score_gain(key, part):
    return jnp.exp(jax.random.uniform(jax.random.fold_in(key, 22), (HEADS,), jnp.float32, jnp.log(0.7), jnp.log(2.5)))


def steps_of(stream_key, shape, cuts, smallest, largest):
    def one(position, parts):
        draws = jax.random.uniform(jax.random.fold_in(jax.random.fold_in(stream_key, 6), position), (parts,), jnp.float32, smallest / len(cuts), largest / len(cuts))
        return jnp.repeat(jnp.exp(draws), shape[position] // parts).reshape((-1,) + (1,) * (len(shape) - position - 1))

    loudness = one(*cuts[0])
    for cut in cuts[1:]:
        loudness = loudness * one(*cut)
    return loudness


def centred(own_key, shape, scale, bound, split=(), kind=jnp.bfloat16):
    array = scale * jax.random.normal(own_key, shape, jnp.float32)
    if split:
        array = array * steps_of(own_key, shape, split, -0.22, 0.18)
    return jnp.clip(array, -bound, bound).astype(kind)


def setup_inputs(seed: int = 0, part: int = 0) -> dict:
    key_of = jax.random.split(jax.random.key(seed), 10)
    part_splits = jax.random.split(jax.random.fold_in(key_of[9], part), 10)
    return {
        "tokens": centred(part_splits[0], (SEQS, SEQ_LEN, WIDTH), 1.0, 6.0, ((0, 16), (1, 16))),
        "forget_offset": draw_forget_offset(jax.random.fold_in(jax.random.fold_in(key_of[9], part), 71), part),
        "q_weight": centred(key_of[2], (WIDTH, HEADS * HEAD_DIM), WIDTH ** -0.5, 0.125, ((1, 16),)),
        "k_weight": centred(key_of[3], (WIDTH, KV_HEADS * HEAD_DIM), WIDTH ** -0.5, 0.125, ((1, 16),)),
        "v_weight": centred(key_of[4], (WIDTH, KV_HEADS * HEAD_DIM), WIDTH ** -0.5, 0.125, ((1, 16),)),
        "forget_weight": centred(key_of[5], (WIDTH, HEADS), WIDTH ** -0.5, 0.125),
        "forget_bias": draw_forget_bias(jax.random.fold_in(key_of[9], 71), part),
        "score_gain": draw_score_gain(jax.random.fold_in(key_of[9], 71), part),
        "out_gain": jnp.clip(1.0 + 0.18 * jax.random.normal(key_of[8], (HEADS * HEAD_DIM,), jnp.float32), 0.1, 1.9),
    }


NEG = -1e+30
QK_FLOOR = 0.1
OUT_FLOOR = 0.001

def head_norm(vectors, floor):
    return vectors * lax.rsqrt(lax.optimization_barrier(jnp.mean(vectors * vectors, axis=-1, keepdims=True)) + floor)

def attend_sequence(token_rows, offset_rows, q_weight, k_weight, v_weight, forget_weight, forget_bias, score_gain, out_gain):
    length = token_rows.shape[0]
    head_count = forget_bias.shape[0]
    head_dim = out_gain.shape[0] // head_count
    kv_heads = k_weight.shape[1] // head_dim
    group_size = head_count // kv_heads
    queries = jnp.dot(token_rows, q_weight, preferred_element_type=jnp.float32).astype(jnp.bfloat16)
    keys_proj = jnp.dot(token_rows, k_weight, preferred_element_type=jnp.float32).astype(jnp.bfloat16)
    values_proj = jnp.dot(token_rows, v_weight, preferred_element_type=jnp.float32).astype(jnp.bfloat16)
    forget_input = (jnp.dot(token_rows, forget_weight, preferred_element_type=jnp.float32) + offset_rows[:, None]).astype(jnp.bfloat16)
    log_gate = jax.nn.log_sigmoid(forget_input.astype(jnp.float32) + forget_bias[None, :])
    cumulative = jnp.cumsum(log_gate, axis=0).reshape(length, kv_heads, group_size)
    query_unit = head_norm(queries.astype(jnp.float32).reshape(length, kv_heads, group_size, head_dim), QK_FLOOR).astype(jnp.bfloat16)
    key_unit = head_norm(keys_proj.astype(jnp.float32).reshape(length, kv_heads, head_dim), QK_FLOOR).astype(jnp.bfloat16)
    value_heads = values_proj.reshape(length, kv_heads, head_dim)
    factor = (score_gain * head_dim ** (-0.5)).reshape(kv_heads, group_size)
    out_gains = out_gain.reshape(kv_heads, group_size, head_dim)
    span_rows = 512 if length % 512 == 0 else length
    positions = jnp.arange(length, dtype=jnp.int32)
    key_totals = jnp.transpose(cumulative, (1, 2, 0))

    def one_block(block_index):
        first = (block_index * span_rows).astype(jnp.int32)
        query_block = lax.dynamic_slice_in_dim(query_unit, first, span_rows, 0)
        query_totals = lax.dynamic_slice_in_dim(cumulative, first, span_rows, 0)
        scores = jnp.einsum('qkgd,skd->kgqs', query_block.astype(jnp.float32), key_unit.astype(jnp.float32))
        scores = scores * factor[:, :, None, None] + jnp.transpose(query_totals, (1, 2, 0))[..., None] - key_totals[:, :, None, :]
        allowed = positions[None, :] <= (first + jnp.arange(span_rows, dtype=jnp.int32))[:, None]
        scores = jnp.where(allowed[None, None], scores, NEG)
        row_peak = lax.optimization_barrier(jnp.max(scores, axis=-1, keepdims=True))
        exponent = jnp.exp(scores - row_peak)
        weights = (exponent / lax.optimization_barrier(jnp.sum(exponent, axis=-1, keepdims=True))).astype(jnp.bfloat16)
        mixed = jnp.einsum('kgqs,skd->qkgd', weights.astype(jnp.float32), value_heads.astype(jnp.float32))
        return (head_norm(mixed, OUT_FLOOR) * out_gains).astype(jnp.bfloat16)
    outputs = lax.map(one_block, jnp.arange(length // span_rows, dtype=jnp.int32))
    return outputs.reshape(length, head_count * head_dim)

def reference(tokens, forget_offset, q_weight, k_weight, v_weight, forget_weight, forget_bias, score_gain, out_gain):

    def attend_one(one_pair):
        return attend_sequence(one_pair[0], one_pair[1], q_weight, k_weight, v_weight, forget_weight, forget_bias, score_gain, out_gain)
    return lax.map(attend_one, (tokens, forget_offset))
```

```python
import functools

import jax
import jax.numpy as jnp
from jax import lax
from jax.experimental import pallas as pl
from jax.experimental.pallas import tpu as pltpu
from jax.sharding import PartitionSpec as P

NEG = -1e30
QK_FLOOR = 0.1
OUT_FLOOR = 0.001
PAD = 8
BACK = 5


NT = (((1,), (1,)), ((), ()))
VM = pl.BlockSpec(memory_space=pltpu.VMEM)
SM = pl.BlockSpec(memory_space=pltpu.SMEM)


def unit(vectors):
    wide = vectors.astype(jnp.float32)
    mean = jnp.mean(wide * wide, axis=-1, keepdims=True)
    return (wide * lax.rsqrt(mean + QK_FLOOR)).astype(jnp.bfloat16)


def pack_kernel(x_ref, kv_ref, gate_ref, shift_ref, out_ref):
    g = pl.program_id(0)
    x = x_ref[...]
    rows = x.shape[0]
    width = x.shape[1]
    head_dim = kv_ref.shape[0]
    keys = lax.dot_general(x, kv_ref[:, :width], NT, preferred_element_type=jnp.float32)
    values = lax.dot_general(x, kv_ref[:, width:], NT, preferred_element_type=jnp.float32)
    at = pl.multiple_of(g * 2 * rows, 2 * rows)
    out_ref[pl.ds(at, rows), :] = unit(keys.astype(jnp.bfloat16))
    out_ref[pl.ds(at + rows, rows), :] = values.astype(jnp.bfloat16)

    @pl.when(g == 0)
    def _():
        gates = lax.dot_general(gate_ref[...], x, NT, preferred_element_type=jnp.float32)
        base = pl.num_programs(0) * 2 * rows
        out_ref[pl.ds(base, gates.shape[0]), :] = (gates + shift_ref[...]).astype(jnp.bfloat16)


def query_kernel(x_ref, w_ref, out_ref):
    for i in range(w_ref.shape[0]):
        out_ref[i] = unit(
            jnp.dot(x_ref[...], w_ref[i], preferred_element_type=jnp.float32).astype(jnp.bfloat16)
        )


def attend_kernel(n, z_ref, fac_ref, q_ref, bias_ref, gain_ref, *rest):
    blocks, gates = rest[:n], rest[n : 2 * n]
    out_ref, bias_of, own_of, s_ref, m_ref, l_ref, acc_ref = rest[2 * n :]
    g = pl.program_id(0)
    z = z_ref[0]
    group, rows, dim = q_ref.shape

    @pl.when(g == 0)
    def _():
        lane = lax.broadcasted_iota(jnp.int32, own_of.shape, 1)
        run = jnp.zeros((own_of.shape[0], 1), jnp.float32)
        for k in range(n):
            gate = jax.nn.log_sigmoid(gates[k][...].astype(jnp.float32) + bias_ref[...])
            step = 1
            while step < rows:
                gate = gate + jnp.where(lane >= step, pltpu.roll(gate, step, 1), 0.0)
                step *= 2
            if k == 0:
                own_of[...] = gate
                bias_of[0] = -gate
            else:
                run = run + gate[:, rows - 1 :]
                bias_of[k] = jnp.where(z >= k, run - gate, NEG)

    row = lax.broadcasted_iota(jnp.int32, (rows, rows), 0)
    col = lax.broadcasted_iota(jnp.int32, (rows, rows), 1)
    here = pl.ds(pl.multiple_of(g * PAD, PAD), PAD)
    own = own_of[here, :]
    columns = [
        jnp.sum(jnp.where(row == col, own[i : i + 1, :], 0.0), axis=1, keepdims=True)
        for i in range(group)
    ]
    queries = q_ref[...].reshape(group * rows, dim)
    m_ref[...] = jnp.full(m_ref.shape, NEG, jnp.float32)

    def score(p):
        keys = jnp.concatenate([blocks[2 * p][:rows, :], blocks[2 * p + 1][:rows, :]], axis=0)
        dots = lax.dot_general(queries, keys, NT, preferred_element_type=jnp.float32)
        near, far = bias_of[2 * p, here, :], bias_of[2 * p + 1, here, :]
        for i in range(group):
            mine = slice(i * rows, (i + 1) * rows)
            factor = fac_ref[g * group + i]
            a = dots[mine, :rows] * factor + (columns[i] + near[i : i + 1, :])
            b = dots[mine, rows:] * factor + (columns[i] + far[i : i + 1, :])
            if p == 0:
                a = jnp.where(col <= row, a, NEG)
            s_ref[p, mine, :rows] = a
            s_ref[p, mine, rows:] = b
            m_ref[mine, :] = jnp.maximum(m_ref[mine, :], jnp.maximum(a, b))

    def mix(p):
        values = jnp.concatenate([blocks[2 * p][rows:, :], blocks[2 * p + 1][rows:, :]], axis=0)
        for i in range(group):
            mine = slice(i * rows, (i + 1) * rows)
            e = jnp.exp(s_ref[p, mine, :] - m_ref[mine, :1])
            total = e[:, :rows] + e[:, rows:]
            mixed = jnp.dot(e.astype(jnp.bfloat16), values, preferred_element_type=jnp.float32)
            if p == 0:
                l_ref[mine, :] = total
                acc_ref[mine, :] = mixed
            else:
                l_ref[mine, :] += total
                acc_ref[mine, :] += mixed

    score(0)
    for p in range(1, n // 2):
        pl.when(z >= 2 * p)(functools.partial(score, p))
    m_ref[...] = jnp.broadcast_to(jnp.max(m_ref[...], axis=1, keepdims=True), m_ref.shape)
    mix(0)
    for p in range(1, n // 2):
        pl.when(z >= 2 * p)(functools.partial(mix, p))
    for i in range(group):
        mine = slice(i * rows, (i + 1) * rows)
        mixed = acc_ref[mine, :] / jnp.sum(l_ref[mine, :], axis=1, keepdims=True)
        mean = jnp.mean(mixed * mixed, axis=-1, keepdims=True)
        scaled = mixed * lax.rsqrt(mean + OUT_FLOOR) * gain_ref[:, i * dim : (i + 1) * dim]
        out_ref[:, i * dim : (i + 1) * dim] = scaled.astype(jnp.bfloat16)


def local(
    tokens,
    forget_offset,
    q_weight,
    k_weight,
    v_weight,
    forget_weight,
    forget_bias,
    score_gain,
    out_gain,
):
    x = tokens[0]
    rows, width = x.shape
    heads = forget_bias.shape[0]
    dim = out_gain.shape[0] // heads
    n = lax.axis_size("sp")
    kv_heads = k_weight.shape[1] * lax.axis_size("dp") // dim
    group = heads // kv_heads
    z = lax.axis_index("sp").astype(jnp.int32).reshape(1)

    def padded(a):
        a = a.reshape(kv_heads, group, *a.shape[1:])
        return jnp.pad(a, ((0, 0), (0, PAD - group), (0, 0))).reshape(kv_heads * PAD, -1)

    gate_weight = padded(forget_weight.T)
    gate_bias = padded(forget_bias[:, None])
    gate_rows = kv_heads * PAD

    kv_own = jnp.concatenate([k_weight.T, v_weight.T], axis=1)
    kv_weight = lax.all_gather(kv_own, "dp", axis=0, tiled=True)
    q_own, kv_weight = lax.optimization_barrier((q_weight, kv_weight))
    q_all = lax.all_gather(q_own, "dp", axis=0, tiled=False)

    block_rows = kv_heads * 2 * rows + gate_rows
    block = pl.pallas_call(
        pack_kernel,
        grid=(kv_heads,),
        in_specs=[
            pl.BlockSpec((rows, width), lambda g: (0, 0)),
            pl.BlockSpec((dim, 2 * width), lambda g: (g, 0)),
            pl.BlockSpec((gate_rows, width), lambda g: (0, 0)),
            pl.BlockSpec((1, rows), lambda g: (0, 0)),
        ],
        out_specs=pl.BlockSpec((block_rows, dim), lambda g: (0, 0)),
        out_shape=jax.ShapeDtypeStruct((block_rows, dim), jnp.bfloat16),
        cost_estimate=pl.CostEstimate(
            flops=4 * rows * width * kv_heads * dim, bytes_accessed=6 << 20, transcendentals=0
        ),
        name="pack",
    )(x, kv_weight, gate_weight, forget_offset)

    upward = n - 1 - BACK
    chain = [block] + [None] * (n - 1)
    up = down = block
    for k in range(1, upward + 1):
        up = lax.ppermute(up, "sp", [(i, i + 1) for i in range(k - 1, n - 1)])
        chain[k] = up
        if k <= BACK:
            senders = [(b - k + 1) % n for b in range(BACK)]
            down = lax.ppermute(down, "sp", [(i, (i - 1) % n) for i in senders])
            chain[n - k] = down

    q_all, _ = lax.optimization_barrier((q_all, chain[max(1, upward - 3)]))
    step = 2
    queries = pl.pallas_call(
        query_kernel,
        grid=(heads // step,),
        in_specs=[
            pl.BlockSpec((rows, width), lambda h: (0, 0)),
            pl.BlockSpec((step, width, dim), lambda h: (h, 0, 0)),
        ],
        out_specs=pl.BlockSpec((step, rows, dim), lambda h: (h, 0, 0)),
        out_shape=jax.ShapeDtypeStruct((heads, rows, dim), jnp.bfloat16),
        cost_estimate=pl.CostEstimate(
            flops=2 * rows * width * heads * dim, bytes_accessed=9 << 20, transcendentals=0
        ),
        name="query",
    )(x, q_all)

    gates_at = (block_rows - gate_rows) // gate_rows
    f32 = jnp.float32
    attended = pl.pallas_call(
        functools.partial(attend_kernel, n),
        grid=(kv_heads,),
        in_specs=[
            SM,
            SM,
            pl.BlockSpec((group, rows, dim), lambda g: (g, 0, 0)),
            pl.BlockSpec((gate_rows, 1), lambda g: (0, 0)),
            pl.BlockSpec((1, group * dim), lambda g: (0, g)),
        ]
        + [pl.BlockSpec((2 * rows, dim), lambda g: (g, 0))] * n
        + [pl.BlockSpec((gate_rows, dim), lambda g: (gates_at, 0))] * n,
        out_specs=pl.BlockSpec((rows, group * dim), lambda g: (0, g)),
        out_shape=jax.ShapeDtypeStruct((rows, heads * dim), jnp.bfloat16),
        scratch_shapes=[
            pltpu.VMEM((n, gate_rows, rows), f32),
            pltpu.VMEM((gate_rows, rows), f32),
            pltpu.VMEM((n // 2, group * rows, 2 * rows), f32),
            pltpu.VMEM((group * rows, rows), f32),
            pltpu.VMEM((group * rows, rows), f32),
            pltpu.VMEM((group * rows, dim), f32),
        ],
        cost_estimate=pl.CostEstimate(
            flops=4 * rows * n * rows * heads * dim, bytes_accessed=5 << 20, transcendentals=1 << 22
        ),
        name="attend",
    )(z, score_gain * dim**-0.5, queries, gate_bias, out_gain[None, :], *chain, *chain)
    return attended[None]


def solution(mesh):
    in_specs = (
        P(("grp", "dp"), "sp", None),
        P(("grp", "dp"), "sp"),
        P(None, "dp"),
        P(None, "dp"),
        P(None, "dp"),
        P(),
        P(),
        P(),
        P(),
    )
    out_specs = P(("grp", "dp"), "sp", None)
    return jax.shard_map(local, mesh=mesh, in_specs=in_specs, out_specs=out_specs, check_vma=False)
```

```python
import functools

import jax
import jax.numpy as jnp
from jax import lax
from jax.experimental import pallas as pl
from jax.experimental.pallas import tpu as pltpu
from jax.sharding import PartitionSpec as P

NEG = -1e30
QK_FLOOR = 0.1
OUT_FLOOR = 0.001
LOG2_E = 1.4426950408889634
PAD = 8
BACK = 6


NT = (((1,), (1,)), ((), ()))
VM = pl.BlockSpec(memory_space=pltpu.VMEM)
SM = pl.BlockSpec(memory_space=pltpu.SMEM)


def unit(vectors):
    wide = vectors.astype(jnp.float32)
    mean = jnp.mean(wide * wide, axis=-1, keepdims=True)
    return (wide * lax.rsqrt(mean + QK_FLOOR)).astype(jnp.bfloat16)


def pack_kernel(x_ref, kv_ref, gate_ref, shift_ref, out_ref):
    g = pl.program_id(0)
    x = x_ref[...]
    rows, width = x.shape
    dim = kv_ref.shape[0]
    both = jnp.concatenate([kv_ref[:, :width], kv_ref[:, width:]], axis=0)
    made = lax.dot_general(x, both, NT, preferred_element_type=jnp.float32).astype(jnp.bfloat16)
    at = pl.multiple_of(g * 2 * rows, 2 * rows)
    out_ref[pl.ds(at, rows), :] = unit(made[:, :dim])
    out_ref[pl.ds(at + rows, rows), :] = made[:, dim:]

    @pl.when(g == 0)
    def _():
        gates = lax.dot_general(gate_ref[...], x, NT, preferred_element_type=jnp.float32)
        base = pl.num_programs(0) * 2 * rows
        out_ref[pl.ds(base, gates.shape[0]), :] = (gates + shift_ref[...]).astype(jnp.bfloat16)


def query_kernel(x_ref, w_ref, out_ref):
    dim = w_ref.shape[2]
    for i in range(0, w_ref.shape[0], 2):
        two = jnp.concatenate([w_ref[i], w_ref[i + 1]], axis=1)
        made = jnp.dot(x_ref[...], two, preferred_element_type=jnp.float32).astype(jnp.bfloat16)
        out_ref[i] = unit(made[:, :dim])
        out_ref[i + 1] = unit(made[:, dim:])


def attend_kernel(n, z_ref, fac_ref, q_ref, bias_ref, gain_ref, *rest):
    blocks = rest[:n]
    out_ref, bias_of, own_of, s_ref, m_ref, l_ref, acc_ref = rest[n:]
    z = z_ref[0]
    heads, rows, dim = q_ref.shape
    gate_rows = own_of.shape[0]
    groups = gate_rows // PAD
    group = heads // groups
    gates_at = groups * 2 * rows

    lane = lax.broadcasted_iota(jnp.int32, own_of.shape, 1)
    run = jnp.zeros((gate_rows, 1), jnp.float32)
    for k in range(n):
        gate = blocks[k][gates_at : gates_at + gate_rows, :].astype(jnp.float32)
        gate = jax.nn.log_sigmoid(gate + bias_ref[...]) * LOG2_E
        step = 1
        while step < rows:
            gate = gate + jnp.where(lane >= step, pltpu.roll(gate, step, 1), 0.0)
            step *= 2
        if k == 0:
            own_of[...] = gate
            bias_of[0] = -gate
        else:
            run = run + gate[:, rows - 1 :]
            bias_of[k] = jnp.where(z >= k, run - gate, NEG)

    row = lax.broadcasted_iota(jnp.int32, (rows, rows), 0)
    col = lax.broadcasted_iota(jnp.int32, (rows, rows), 1)
    bodies, k = [], 0
    while k < n:
        size = min(2 if k < 4 else 4, n - k)
        bodies.append((k, size))
        k += size

    def one_group(g, carry):
        here = pl.ds(pl.multiple_of(g * PAD, PAD), PAD)
        keys_at = pl.ds(pl.multiple_of(g * 2 * rows, 2 * rows), rows)
        values_at = pl.ds(pl.multiple_of(g * 2 * rows + rows, rows), rows)
        own = own_of[here, :]
        columns = [
            jnp.sum(jnp.where(row == col, own[i : i + 1, :], 0.0), axis=1, keepdims=True)
            for i in range(group)
        ]
        queries = q_ref[pl.ds(g * group, group)].reshape(group * rows, dim)

        def score(first, size):
            keys = jnp.concatenate([blocks[first + j][keys_at, :] for j in range(size)], axis=0)
            dots = lax.dot_general(queries, keys, NT, preferred_element_type=jnp.float32)
            biases = [bias_of[first + j, here, :] for j in range(size)]
            for i in range(group):
                mine = slice(i * rows, (i + 1) * rows)
                factor = fac_ref[g * group + i]
                most = None if first == 0 else m_ref[mine, :]
                for j in range(size):
                    part = dots[mine, j * rows : (j + 1) * rows] * factor
                    part = part + (columns[i] + biases[j][i : i + 1, :])
                    if first + j == 0:
                        part = jnp.where(col <= row, part, NEG)
                    s_ref[first + j, mine, :] = part
                    most = part if most is None else jnp.maximum(most, part)
                m_ref[mine, :] = most

        def mix(first, size):
            values = jnp.concatenate([blocks[first + j][values_at, :] for j in range(size)], axis=0)
            for i in range(group):
                mine = slice(i * rows, (i + 1) * rows)
                top = m_ref[mine, :]
                es = [jnp.exp2(s_ref[first + j, mine, :] - top) for j in range(size)]
                total = functools.reduce(jnp.add, es)
                weights = jnp.concatenate([e.astype(jnp.bfloat16) for e in es], axis=1)
                mixed = jnp.dot(weights, values, preferred_element_type=jnp.float32)
                if first == 0:
                    l_ref[mine, :] = total
                    acc_ref[mine, :] = mixed
                else:
                    l_ref[mine, :] += total
                    acc_ref[mine, :] += mixed

        score(*bodies[0])
        for first, size in bodies[1:]:
            pl.when(z >= first)(functools.partial(score, first, size))
        m_ref[...] = jnp.broadcast_to(jnp.max(m_ref[...], axis=1, keepdims=True), m_ref.shape)
        mix(*bodies[0])
        for first, size in bodies[1:]:
            pl.when(z >= first)(functools.partial(mix, first, size))
        for i in range(group):
            mine = slice(i * rows, (i + 1) * rows)
            mixed = acc_ref[mine, :] / jnp.sum(l_ref[mine, :], axis=1, keepdims=True)
            mean = jnp.mean(mixed * mixed, axis=-1, keepdims=True)
            head = pl.ds(pl.multiple_of((g * group + i) * dim, dim), dim)
            scaled = mixed * lax.rsqrt(mean + OUT_FLOOR) * gain_ref[:, head]
            out_ref[:, head] = scaled.astype(jnp.bfloat16)
        return carry

    lax.fori_loop(0, groups, one_group, 0)


def local(
    tokens,
    forget_offset,
    q_weight,
    k_weight,
    v_weight,
    forget_weight,
    forget_bias,
    score_gain,
    out_gain,
):
    x = tokens[0]
    rows, width = x.shape
    heads = forget_bias.shape[0]
    dim = out_gain.shape[0] // heads
    n = lax.axis_size("sp")
    kv_heads = k_weight.shape[1] * lax.axis_size("dp") // dim
    group = heads // kv_heads
    z = lax.axis_index("sp").astype(jnp.int32).reshape(1)

    def padded(a):
        a = a.reshape(kv_heads, group, *a.shape[1:])
        return jnp.pad(a, ((0, 0), (0, PAD - group), (0, 0))).reshape(kv_heads * PAD, -1)

    gate_weight = padded(forget_weight.T)
    gate_bias = padded(forget_bias[:, None])
    gate_rows = kv_heads * PAD

    kv_own = jnp.concatenate([k_weight.T, v_weight.T], axis=1)
    kv_weight = lax.all_gather(kv_own, "dp", axis=0, tiled=True)
    q_own, kv_weight = lax.optimization_barrier((q_weight, kv_weight))
    q_all = lax.all_gather(q_own, "dp", axis=0, tiled=False)

    block_rows = kv_heads * 2 * rows + gate_rows
    block = pl.pallas_call(
        pack_kernel,
        grid=(kv_heads,),
        in_specs=[
            pl.BlockSpec((rows, width), lambda g: (0, 0)),
            pl.BlockSpec((dim, 2 * width), lambda g: (g, 0)),
            pl.BlockSpec((gate_rows, width), lambda g: (0, 0)),
            pl.BlockSpec((1, rows), lambda g: (0, 0)),
        ],
        out_specs=pl.BlockSpec((block_rows, dim), lambda g: (0, 0)),
        out_shape=jax.ShapeDtypeStruct((block_rows, dim), jnp.bfloat16),
        cost_estimate=pl.CostEstimate(
            flops=4 * rows * width * kv_heads * dim, bytes_accessed=6 << 20, transcendentals=0
        ),
        compiler_params=pltpu.CompilerParams(vmem_limit_bytes=60 << 20),
        name="pack",
    )(x, kv_weight, gate_weight, forget_offset)

    upward = n - 1 - BACK
    chain = [block] + [None] * (n - 1)
    up = down = block
    for k in range(1, upward + 1):
        if k <= BACK:
            senders = [(b - k + 1) % n for b in range(BACK)]
            new_down = lax.ppermute(down, "sp", [(i, (i - 1) % n) for i in senders])
        up = lax.ppermute(up, "sp", [(i, i + 1) for i in range(k - 1, n - 1)])
        if k <= BACK:
            up, down = lax.optimization_barrier((up, new_down))
            chain[n - k] = down
        chain[k] = up

    q_all, _ = lax.optimization_barrier((q_all, chain[max(1, upward - 2)]))
    step = 2
    queries = pl.pallas_call(
        query_kernel,
        grid=(heads // step,),
        in_specs=[
            pl.BlockSpec((rows, width), lambda h: (0, 0)),
            pl.BlockSpec((step, width, dim), lambda h: (h, 0, 0)),
        ],
        out_specs=pl.BlockSpec((step, rows, dim), lambda h: (h, 0, 0)),
        out_shape=jax.ShapeDtypeStruct((heads, rows, dim), jnp.bfloat16),
        cost_estimate=pl.CostEstimate(
            flops=2 * rows * width * heads * dim, bytes_accessed=9 << 20, transcendentals=0
        ),
        compiler_params=pltpu.CompilerParams(vmem_limit_bytes=56 << 20),
        name="query",
    )(x, q_all)

    f32 = jnp.float32
    attended = pl.pallas_call(
        functools.partial(attend_kernel, n),
        in_specs=[SM, SM] + [VM] * (3 + n),
        out_specs=VM,
        out_shape=jax.ShapeDtypeStruct((rows, heads * dim), jnp.bfloat16),
        scratch_shapes=[
            pltpu.VMEM((n, gate_rows, rows), f32),
            pltpu.VMEM((gate_rows, rows), f32),
            pltpu.VMEM((n, group * rows, rows), f32),
            pltpu.VMEM((group * rows, rows), f32),
            pltpu.VMEM((group * rows, rows), f32),
            pltpu.VMEM((group * rows, dim), f32),
        ],
        cost_estimate=pl.CostEstimate(
            flops=4 * rows * n * rows * heads * dim, bytes_accessed=5 << 20, transcendentals=1 << 22
        ),
        compiler_params=pltpu.CompilerParams(vmem_limit_bytes=16 << 20),
        name="attend",
    )(z, score_gain * (dim**-0.5 * LOG2_E), queries, gate_bias, out_gain[None, :], *chain)
    return attended[None]


def solution(mesh):
    in_specs = (
        P(("grp", "dp"), "sp", None),
        P(("grp", "dp"), "sp"),
        P(None, "dp"),
        P(None, "dp"),
        P(None, "dp"),
        P(),
        P(),
        P(),
        P(),
    )
    out_specs = P(("grp", "dp"), "sp", None)
    return jax.shard_map(local, mesh=mesh, in_specs=in_specs, out_specs=out_specs, check_vma=False)
```

```python
import functools

import jax
import jax.numpy as jnp
from jax import lax
from jax.experimental import pallas as pl
from jax.experimental.pallas import tpu as pltpu
from jax.sharding import PartitionSpec as P

NEG = -1e30
QK_FLOOR = 0.1
OUT_FLOOR = 0.001
LOG2_E = 1.4426950408889634
PAD = 8
BACK = 7


NT = (((1,), (1,)), ((), ()))
VM = pl.BlockSpec(memory_space=pltpu.VMEM)
SM = pl.BlockSpec(memory_space=pltpu.SMEM)


def unit(vectors, axis):
    wide = vectors.astype(jnp.float32)
    mean = jnp.mean(wide * wide, axis=axis, keepdims=True)
    return wide * lax.rsqrt(mean + QK_FLOOR)


def pack_kernel(x_ref, gate_ref, shift_ref, first_ref, second_ref):
    half = second_ref.shape[0]
    rows = x_ref.shape[0]
    first_ref[:half, :] = x_ref[:half, :]
    second_ref[...] = x_ref[half:, :]
    gates = lax.dot_general(gate_ref[...], x_ref[...], NT, preferred_element_type=jnp.float32)
    gates = (gates + shift_ref[...]).astype(jnp.bfloat16)
    first_ref[half:, :] = jnp.zeros((PAD, first_ref.shape[1]), jnp.bfloat16)
    for g in range(gates.shape[0] // PAD):
        first_ref[half:, g * rows : (g + 1) * rows] = gates[g * PAD : (g + 1) * PAD, :]


def layer_kernel(n, z_ref, fac_ref, x_ref, bias_ref, gain_ref, w_ref, *rest):
    firsts, seconds = rest[:n], rest[n : 2 * n]
    (out_ref, q_w, kv_w, q_of, kv_of, bias_of, own_of, s_ref, m_ref, l_ref, acc_ref) = rest[
        2 * n : 2 * n + 11
    ]
    x_of, gates_of, q_sem, kv_sem, x_sem, gates_sem = rest[2 * n + 11 :]
    z = z_ref[0]
    rows = x_ref.shape[0]
    group, dim = q_w.shape[1:3]
    half = seconds[0].shape[0]
    gate_rows = own_of.shape[0]
    groups = gate_rows // PAD

    def fetch(g, slot):
        mine = pl.ds(g * group, group)
        return (
            pltpu.make_async_copy(w_ref.at[mine, pl.ds(0, dim), :], q_w.at[slot], q_sem.at[slot]),
            pltpu.make_async_copy(
                w_ref.at[mine, pl.ds(dim, kv_w.shape[2]), :], kv_w.at[slot], kv_sem.at[slot]
            ),
        )

    def load(k):
        top = pl.ds(k * rows, half)
        low = pl.ds(k * rows + half, half)
        return (
            pltpu.make_async_copy(firsts[k].at[pl.ds(0, half), :], x_of.at[top], x_sem.at[k, 0]),
            pltpu.make_async_copy(seconds[k], x_of.at[low], x_sem.at[k, 1]),
        )

    def load_gates(k):
        return pltpu.make_async_copy(
            firsts[k].at[pl.ds(half, PAD), pl.ds(0, gates_of.shape[2])],
            gates_of.at[k],
            gates_sem.at[k],
        )

    bodies, k = [], 0
    while k < n:
        size = min(2 if k < 4 else 4, n - k)
        bodies.append((k, size))
        k += size

    def blocks_of(first, size, act):
        for k in range(first, first + size):
            for copy in load(k):
                act(copy)

    for k in range(n):
        load_gates(k).start()
    for copy in fetch(0, 0):
        copy.start()
    blocks_of(*bodies[0], lambda copy: copy.start())
    for first, size in bodies[1:]:
        pl.when(z >= first)(functools.partial(blocks_of, first, size, lambda copy: copy.start()))
    for k in range(n):
        load_gates(k).wait()

    gates = [
        gates_of[k, :, g * rows : (g + 1) * rows].astype(jnp.float32)
        for k in range(n)
        for g in range(groups)
    ]
    gates = jnp.concatenate(gates, axis=0) + jnp.concatenate([bias_ref[...]] * n, axis=0)
    gates = jax.nn.log_sigmoid(gates) * LOG2_E
    lane = lax.broadcasted_iota(jnp.int32, gates.shape, 1)
    step = 1
    while step < rows:
        gates = gates + jnp.where(lane >= step, pltpu.roll(gates, step, 1), 0.0)
        step *= 2
    run = jnp.zeros((gate_rows, 1), jnp.float32)
    for k in range(n):
        gate = gates[k * gate_rows : (k + 1) * gate_rows, :]
        if k == 0:
            own_of[...] = gate
            bias_of[0] = -gate
        else:
            run = run + gate[:, rows - 1 :]
            bias_of[k] = jnp.where(z >= k, run - gate, NEG)

    row = lax.broadcasted_iota(jnp.int32, (rows, rows), 0)
    col = lax.broadcasted_iota(jnp.int32, (rows, rows), 1)
    def one_group(g, carry):
        slot = lax.rem(g, 2)
        for copy in fetch(g, slot):
            copy.wait()

        @pl.when(g + 1 < groups)
        def _():
            for copy in fetch(g + 1, 1 - slot):
                copy.start()

        here = pl.ds(pl.multiple_of(g * PAD, PAD), PAD)
        own = own_of[here, :]
        columns = [
            jnp.sum(jnp.where(row == col, own[i : i + 1, :], 0.0), axis=1, keepdims=True)
            for i in range(group)
        ]
        made = lax.dot_general(
            q_w[slot].reshape(group * dim, q_w.shape[3]),
            x_ref[...],
            NT,
            preferred_element_type=jnp.float32,
        ).astype(jnp.bfloat16)
        for i in range(group):
            turned = unit(made[i * dim : (i + 1) * dim, :], 0).T
            q_of[i * rows : (i + 1) * rows, :] = turned.astype(jnp.bfloat16)
        piece = kv_w.shape[2] // 2
        weights = jnp.concatenate(
            [kv_w[slot, i, :piece, :] for i in range(group)]
            + [kv_w[slot, i, piece:, :] for i in range(group)],
            axis=0,
        )

        def score(first, size):
            pl.when(g == 0)(functools.partial(blocks_of, first, size, lambda copy: copy.wait()))
            made = lax.dot_general(
                x_of[first * rows : (first + size) * rows, :],
                weights,
                NT,
                preferred_element_type=jnp.float32,
            ).astype(jnp.bfloat16)
            keys = unit(made[:, :dim], 1).astype(jnp.bfloat16)
            for j in range(size):
                kv_of[first + j] = made[j * rows : (j + 1) * rows, dim:]
            dots = lax.dot_general(q_of[...], keys, NT, preferred_element_type=jnp.float32)
            biases = [bias_of[first + j, here, :] for j in range(size)]
            for i in range(group):
                mine = slice(i * rows, (i + 1) * rows)
                factor = fac_ref[g * group + i]
                most = None if first == 0 else m_ref[mine, :]
                for j in range(size):
                    part = dots[mine, j * rows : (j + 1) * rows] * factor
                    part = part + (columns[i] + biases[j][i : i + 1, :])
                    if first + j == 0:
                        part = jnp.where(col <= row, part, NEG)
                    s_ref[first + j, mine, :] = part
                    most = part if most is None else jnp.maximum(most, part)
                m_ref[mine, :] = most

        def mix(first, size):
            values = jnp.concatenate([kv_of[first + j] for j in range(size)], axis=0)
            for i in range(group):
                mine = slice(i * rows, (i + 1) * rows)
                top = m_ref[mine, :]
                es = [jnp.exp2(s_ref[first + j, mine, :] - top) for j in range(size)]
                total = functools.reduce(jnp.add, es)
                part = jnp.concatenate([e.astype(jnp.bfloat16) for e in es], axis=1)
                mixed = jnp.dot(part, values, preferred_element_type=jnp.float32)
                if first == 0:
                    l_ref[mine, :] = total
                    acc_ref[mine, :] = mixed
                else:
                    l_ref[mine, :] += total
                    acc_ref[mine, :] += mixed

        score(*bodies[0])
        for first, size in bodies[1:]:
            pl.when(z >= first)(functools.partial(score, first, size))
        m_ref[...] = jnp.broadcast_to(jnp.max(m_ref[...], axis=1, keepdims=True), m_ref.shape)
        mix(*bodies[0])
        for first, size in bodies[1:]:
            pl.when(z >= first)(functools.partial(mix, first, size))
        for i in range(group):
            mine = slice(i * rows, (i + 1) * rows)
            mixed = acc_ref[mine, :] / jnp.sum(l_ref[mine, :], axis=1, keepdims=True)
            mean = jnp.mean(mixed * mixed, axis=-1, keepdims=True)
            head = pl.ds(pl.multiple_of((g * group + i) * dim, dim), dim)
            scaled = mixed * lax.rsqrt(mean + OUT_FLOOR) * gain_ref[:, head]
            out_ref[:, head] = scaled.astype(jnp.bfloat16)
        return carry

    lax.fori_loop(0, groups, one_group, 0)


def local(
    tokens,
    forget_offset,
    q_weight,
    k_weight,
    v_weight,
    forget_weight,
    forget_bias,
    score_gain,
    out_gain,
):
    x = tokens[0]
    rows, width = x.shape
    half = rows // 2
    heads = forget_bias.shape[0]
    dim = out_gain.shape[0] // heads
    n = lax.axis_size("sp")
    parts = lax.axis_size("dp")
    kv_heads = k_weight.shape[1] * parts // dim
    group = heads // kv_heads
    piece = 2 * k_weight.shape[1]
    z = lax.axis_index("sp").astype(jnp.int32).reshape(1)
    bf16, f32 = jnp.bfloat16, jnp.float32

    def padded(a):
        a = a.reshape(kv_heads, group, *a.shape[1:])
        return jnp.pad(a, ((0, 0), (0, PAD - group), (0, 0))).reshape(kv_heads * PAD, -1)

    gate_rows = kv_heads * PAD
    weight_own = jnp.concatenate([q_weight.T, k_weight.T, v_weight.T], axis=0)
    weight_all = lax.all_gather(weight_own, "dp", axis=0, tiled=False)

    sent = pl.pallas_call(
        pack_kernel,
        in_specs=[VM, VM, VM],
        out_specs=[VM, VM],
        out_shape=[
            jax.ShapeDtypeStruct((half + PAD, width), bf16),
            jax.ShapeDtypeStruct((half, width), bf16),
        ],
        cost_estimate=pl.CostEstimate(
            flops=2 * rows * width * gate_rows, bytes_accessed=1 << 20, transcendentals=0
        ),
        compiler_params=pltpu.CompilerParams(vmem_limit_bytes=16 << 20),
        name="pack",
    )(x, padded(forget_weight.T), forget_offset)

    upward = n - 1 - BACK
    chains = [[block] + [None] * (n - 1) for block in sent]
    ups, downs = list(sent), list(sent)
    for k in range(1, upward + 1):
        rising = [(i, i + 1) for i in range(k - 1, n - 1)]
        sinking = [((b - k + 1) % n, (b - k) % n) for b in range(BACK)]
        for c, chain in enumerate(chains):
            if k <= BACK:
                down = lax.ppermute(downs[c], "sp", sinking)
            ups[c] = lax.ppermute(ups[c], "sp", rising)
            if k <= BACK:
                ups[c], downs[c] = lax.optimization_barrier((ups[c], down))
                chain[n - k] = downs[c]
            chain[k] = ups[c]

    attended = pl.pallas_call(
        functools.partial(layer_kernel, n),
        in_specs=[SM, SM, VM, VM, VM] + [pl.BlockSpec(memory_space=pltpu.HBM)] * (1 + 2 * n),
        out_specs=VM,
        out_shape=jax.ShapeDtypeStruct((rows, heads * dim), bf16),
        scratch_shapes=[
            pltpu.VMEM((2, group, dim, width), bf16),
            pltpu.VMEM((2, group, piece, width), bf16),
            pltpu.VMEM((group * rows, dim), bf16),
            pltpu.VMEM((n, rows, dim), bf16),
            pltpu.VMEM((n, gate_rows, rows), f32),
            pltpu.VMEM((gate_rows, rows), f32),
            pltpu.VMEM((n, group * rows, rows), f32),
            pltpu.VMEM((group * rows, rows), f32),
            pltpu.VMEM((group * rows, rows), f32),
            pltpu.VMEM((group * rows, dim), f32),
            pltpu.VMEM((n * rows, width), bf16),
            pltpu.VMEM((n, PAD, kv_heads * rows), bf16),
            pltpu.SemaphoreType.DMA((2,)),
            pltpu.SemaphoreType.DMA((2,)),
            pltpu.SemaphoreType.DMA((n, 2)),
            pltpu.SemaphoreType.DMA((n,)),
        ],
        cost_estimate=pl.CostEstimate(
            flops=8 * rows * n * width * heads * dim // 4,
            bytes_accessed=12 << 20,
            transcendentals=1 << 22,
        ),
        compiler_params=pltpu.CompilerParams(vmem_limit_bytes=60 << 20),
        name="layer",
    )(
        z,
        score_gain * (dim**-0.5 * LOG2_E),
        x,
        padded(forget_bias[:, None]),
        out_gain[None, :],
        weight_all,
        *chains[0],
        *chains[1],
    )
    return attended[None]


def solution(mesh):
    in_specs = (
        P(("grp", "dp"), "sp", None),
        P(("grp", "dp"), "sp"),
        P(None, "dp"),
        P(None, "dp"),
        P(None, "dp"),
        P(),
        P(),
        P(),
        P(),
    )
    out_specs = P(("grp", "dp"), "sp", None)
    return jax.shard_map(local, mesh=mesh, in_specs=in_specs, out_specs=out_specs, check_vma=False)
```

```python
import functools

import jax
import jax.numpy as jnp
from jax import lax
from jax.experimental import pallas as pl
from jax.experimental.pallas import tpu as pltpu
from jax.sharding import PartitionSpec as P

NEG = -1e30
QK_FLOOR = 0.1
OUT_FLOOR = 0.001
LOG2_E = 1.4426950408889634
PAD = 8
LAYER_VMEM = 60 << 20
BACK = 6


NT = (((1,), (1,)), ((), ()))
VM = pl.BlockSpec(memory_space=pltpu.VMEM)
SM = pl.BlockSpec(memory_space=pltpu.SMEM)


def unit(vectors, axis):
    wide = vectors.astype(jnp.float32)
    mean = jnp.mean(wide * wide, axis=axis, keepdims=True)
    return wide * lax.rsqrt(mean + QK_FLOOR)


def pack_kernel(x_ref, gate_ref, shift_ref, bias_ref, first_ref, second_ref, wide_ref):
    half = second_ref.shape[0]
    rows = x_ref.shape[0]
    wide_ref[...] = jnp.broadcast_to(bias_ref[...], wide_ref.shape)
    first_ref[:half, :] = x_ref[:half, :]
    second_ref[...] = x_ref[half:, :]
    gates = lax.dot_general(gate_ref[...], x_ref[...], NT, preferred_element_type=jnp.float32)
    gates = (gates + shift_ref[...]).astype(jnp.bfloat16)
    first_ref[half:, :] = jnp.zeros((PAD, first_ref.shape[1]), jnp.bfloat16)
    for g in range(gates.shape[0] // PAD):
        first_ref[half:, g * rows : (g + 1) * rows] = gates[g * PAD : (g + 1) * PAD, :]


def layer_kernel(n, z_ref, fac_ref, bias_ref, gain_ref, weights_ref, *rest):
    firsts, seconds = rest[:n], rest[n : 2 * n]
    out_ref, q_of, k_of, v_of, bias_of, own_of, s_ref, m_ref, l_ref, acc_ref = rest[
        2 * n : 2 * n + 10
    ]
    w_ref, x_of, gates_of, w_sem, x_sem, gates_sem = rest[2 * n + 10 :]
    z = z_ref[0]
    half = seconds[0].shape[0]
    rows = 2 * half
    heads, per_head, width = w_ref.shape
    groups, dim = k_of.shape[:2]
    group = heads // groups
    piece = (per_head - dim) // 2
    gate_rows = own_of.shape[0]

    def pair(first):
        return x_of[first * rows : (first + 2) * rows, :]

    def keep(g, first, parts):
        at = slice(first * rows, (first + 2) * rows)
        keys = jnp.concatenate([part[:piece] for part in parts], axis=0)
        values = jnp.concatenate([part[piece:] for part in parts], axis=0)
        k_of[g, :, at] = unit(keys, 0).astype(jnp.bfloat16)
        v_of[g, :, at] = values

    def fetch(h):
        return pltpu.make_async_copy(weights_ref.at[h], w_ref.at[h], w_sem.at[h])

    def own_pair(g, carry):
        for i in range(group):
            fetch(g * group + i).wait()
        made = lax.dot_general(
            w_ref[pl.ds(g * group, group)].reshape(group * per_head, width),
            pair(0),
            NT,
            preferred_element_type=jnp.float32,
        ).astype(jnp.bfloat16)
        parts = []
        for i in range(group):
            at = i * per_head
            turned = unit(made[at : at + dim, :rows], 0).T
            q_of[g, i * rows : (i + 1) * rows, :] = turned.astype(jnp.bfloat16)
            parts.append(made[at + dim : at + per_head, :])
        keep(g, 0, parts)
        return carry

    def other_pair(first):
        for copy in load(first) + load(first + 1):
            copy.wait()
        made = lax.dot_general(
            w_ref[:, dim:, :].reshape(heads * 2 * piece, width),
            pair(first),
            NT,
            preferred_element_type=jnp.float32,
        ).astype(jnp.bfloat16)
        for g in range(groups):
            parts = [made[h * 2 * piece : (h + 1) * 2 * piece] for h in range(heads)]
            keep(g, first, parts[g * group : (g + 1) * group])

    def load(k):
        top = pl.ds(k * rows, half)
        low = pl.ds(k * rows + half, half)
        return (
            pltpu.make_async_copy(firsts[k].at[pl.ds(0, half), :], x_of.at[top], x_sem.at[k, 0]),
            pltpu.make_async_copy(seconds[k], x_of.at[low], x_sem.at[k, 1]),
        )

    def load_gates(k):
        return pltpu.make_async_copy(
            firsts[k].at[pl.ds(half, PAD), pl.ds(0, gates_of.shape[2])],
            gates_of.at[k],
            gates_sem.at[k],
        )

    def start_pair(first):
        for copy in load(first) + load(first + 1):
            copy.start()

    start_pair(0)
    for h in range(heads):
        fetch(h).start()
    for k in range(n):
        load_gates(k).start()
    for first in range(2, n, 2):
        pl.when(z >= first)(functools.partial(start_pair, first))

    for copy in load(0) + load(1):
        copy.wait()
    lax.fori_loop(0, groups, own_pair, 0)
    for k in range(n):
        load_gates(k).wait()

    gates = [
        gates_of[k, :, g * rows : (g + 1) * rows].astype(jnp.float32)
        for k in range(n)
        for g in range(groups)
    ]
    gates = jnp.concatenate(gates, axis=0) + jnp.concatenate([bias_ref[...]] * n, axis=0)
    gates = jax.nn.log_sigmoid(gates) * LOG2_E
    lane = lax.broadcasted_iota(jnp.int32, gates.shape, 1)
    step = 1
    while step < rows:
        gates = gates + jnp.where(lane >= step, pltpu.roll(gates, step, 1), 0.0)
        step *= 2
    run = jnp.zeros((gate_rows, 1), jnp.float32)
    for k in range(n):
        gate = gates[k * gate_rows : (k + 1) * gate_rows, :]
        if k == 0:
            own_of[...] = gate
            bias_of[0] = -gate
        else:
            run = run + gate[:, rows - 1 :]
            bias_of[k] = jnp.where(z >= k, run - gate, NEG)

    for first in range(2, n, 2):
        pl.when(z >= first)(functools.partial(other_pair, first))

    row = lax.broadcasted_iota(jnp.int32, (rows, rows), 0)
    col = lax.broadcasted_iota(jnp.int32, (rows, rows), 1)
    bodies, k = [], 0
    while k < n:
        size = min(2 if k < 4 or k >= n - 4 else 4, n - k)
        bodies.append((k, size))
        k += size

    def one_group(g, carry):
        here = pl.ds(pl.multiple_of(g * PAD, PAD), PAD)
        own = own_of[here, :]
        columns = [
            jnp.sum(jnp.where(row == col, own[i : i + 1, :], 0.0), axis=1, keepdims=True)
            for i in range(group)
        ]

        def score(first, size):
            keys = k_of[g, :, first * rows : (first + size) * rows]
            dots = jnp.dot(q_of[g], keys, preferred_element_type=jnp.float32)
            biases = [bias_of[first + j, here, :] for j in range(size)]
            for i in range(group):
                mine = slice(i * rows, (i + 1) * rows)
                factor = fac_ref[g * group + i]
                most = None if first == 0 else m_ref[mine, :]
                for j in range(size):
                    part = dots[mine, j * rows : (j + 1) * rows] * factor
                    part = part + (columns[i] + biases[j][i : i + 1, :])
                    if first + j == 0:
                        part = jnp.where(col <= row, part, NEG)
                    s_ref[first + j, mine, :] = part
                    most = part if most is None else jnp.maximum(most, part)
                m_ref[mine, :] = most

        def mix(first, size):
            values = v_of[g, :, first * rows : (first + size) * rows]
            parts = []
            for i in range(group):
                mine = slice(i * rows, (i + 1) * rows)
                top = m_ref[mine, :]
                es = [jnp.exp2(s_ref[first + j, mine, :] - top) for j in range(size)]
                total = functools.reduce(jnp.add, es)
                parts.append(jnp.concatenate([e.astype(jnp.bfloat16) for e in es], axis=1))
                if first == 0:
                    l_ref[mine, :] = total
                else:
                    l_ref[mine, :] += total
            mixed = lax.dot_general(
                jnp.concatenate(parts, axis=0), values, NT, preferred_element_type=jnp.float32
            )
            if first == 0:
                acc_ref[...] = mixed
            else:
                acc_ref[...] += mixed

        score(*bodies[0])
        for first, size in bodies[1:]:
            pl.when(z >= first)(functools.partial(score, first, size))
        m_ref[...] = jnp.broadcast_to(jnp.max(m_ref[...], axis=1, keepdims=True), m_ref.shape)
        mix(*bodies[0])
        for first, size in bodies[1:]:
            pl.when(z >= first)(functools.partial(mix, first, size))
        for i in range(group):
            mine = slice(i * rows, (i + 1) * rows)
            mixed = acc_ref[mine, :] / jnp.sum(l_ref[mine, :], axis=1, keepdims=True)
            mean = jnp.mean(mixed * mixed, axis=-1, keepdims=True)
            head = pl.ds(pl.multiple_of((g * group + i) * dim, dim), dim)
            scaled = mixed * lax.rsqrt(mean + OUT_FLOOR) * gain_ref[:, head]
            out_ref[:, head] = scaled.astype(jnp.bfloat16)
        return carry

    lax.fori_loop(0, groups, one_group, 0)


def layer_call(z, factor, bias, gain, weights, firsts, seconds):
    half, width = seconds[0].shape
    rows = 2 * half
    n = len(firsts)
    gate_rows = bias.shape[0]
    kv_heads = gate_rows // PAD
    heads = weights.shape[0]
    dim = gain.shape[1] // heads
    group = heads // kv_heads
    bf16, f32 = jnp.bfloat16, jnp.float32
    return pl.pallas_call(
        functools.partial(layer_kernel, n),
        in_specs=[SM, SM, VM, VM] + [pl.BlockSpec(memory_space=pltpu.HBM)] * (1 + 2 * n),
        out_specs=VM,
        out_shape=jax.ShapeDtypeStruct((rows, heads * dim), bf16),
        scratch_shapes=[
            pltpu.VMEM((kv_heads, group * rows, dim), bf16),
            pltpu.VMEM((kv_heads, dim, n * rows), bf16),
            pltpu.VMEM((kv_heads, dim, n * rows), bf16),
            pltpu.VMEM((n, gate_rows, rows), f32),
            pltpu.VMEM((gate_rows, rows), f32),
            pltpu.VMEM((n, group * rows, rows), f32),
            pltpu.VMEM((group * rows, rows), f32),
            pltpu.VMEM((group * rows, rows), f32),
            pltpu.VMEM((group * rows, dim), f32),
            pltpu.VMEM(weights.shape, bf16),
            pltpu.VMEM((n * rows, width), bf16),
            pltpu.VMEM((n, PAD, kv_heads * rows), bf16),
            pltpu.SemaphoreType.DMA((heads,)),
            pltpu.SemaphoreType.DMA((n, 2)),
            pltpu.SemaphoreType.DMA((n,)),
        ],
        cost_estimate=pl.CostEstimate(
            flops=2 * rows * n * width * heads * dim,
            bytes_accessed=12 << 20,
            transcendentals=1 << 22,
        ),
        compiler_params=pltpu.CompilerParams(vmem_limit_bytes=LAYER_VMEM),
        name="layer",
    )(z, factor, bias, gain, weights, *firsts, *seconds)


def local(
    tokens,
    forget_offset,
    q_weight,
    k_weight,
    v_weight,
    forget_weight,
    forget_bias,
    score_gain,
    out_gain,
):
    x = tokens[0]
    rows, width = x.shape
    half = rows // 2
    heads = forget_bias.shape[0]
    dim = out_gain.shape[0] // heads
    n = lax.axis_size("sp")
    parts = lax.axis_size("dp")
    kv_heads = k_weight.shape[1] * parts // dim
    group = heads // kv_heads
    piece = 2 * k_weight.shape[1]
    z = lax.axis_index("sp").astype(jnp.int32).reshape(1)
    bf16, f32 = jnp.bfloat16, jnp.float32

    def padded(a):
        a = a.reshape(kv_heads, group, *a.shape[1:])
        return jnp.pad(a, ((0, 0), (0, PAD - group), (0, 0))).reshape(kv_heads * PAD, -1)

    gate_rows = kv_heads * PAD
    weight_own = jnp.concatenate([q_weight.T, k_weight.T, v_weight.T], axis=0)
    weight_all = lax.all_gather(weight_own, "dp", axis=0, tiled=False)

    *sent, bias = pl.pallas_call(
        pack_kernel,
        in_specs=[VM] * 4,
        out_specs=[VM] * 3,
        out_shape=[
            jax.ShapeDtypeStruct((half + PAD, width), bf16),
            jax.ShapeDtypeStruct((half, width), bf16),
            jax.ShapeDtypeStruct((gate_rows, rows), f32),
        ],
        cost_estimate=pl.CostEstimate(
            flops=2 * rows * width * gate_rows, bytes_accessed=1 << 20, transcendentals=0
        ),
        compiler_params=pltpu.CompilerParams(vmem_limit_bytes=16 << 20),
        name="pack",
    )(x, padded(forget_weight.T), forget_offset, padded(forget_bias[:, None]))

    sent, z, factor, bias, gain = lax.optimization_barrier(
        (
            sent,
            z,
            score_gain * (dim**-0.5 * LOG2_E),
            bias,
            out_gain[None, :],
        )
    )

    upward = n - 1 - BACK
    chains = [[block] + [None] * (n - 1) for block in sent]
    ups, downs = list(sent), list(sent)
    for k in range(1, upward + 1):
        rising = [(i, i + 1) for i in range(k - 1, n - 1)]
        sinking = [((b - k + 1) % n, (b - k) % n) for b in range(BACK)]
        for c, chain in enumerate(chains):
            if k <= BACK:
                down = lax.ppermute(downs[c], "sp", sinking)
            ups[c] = lax.ppermute(ups[c], "sp", rising)
            if k <= BACK:
                ups[c], downs[c] = lax.optimization_barrier((ups[c], down))
                chain[n - k] = downs[c]
            chain[k] = ups[c]

    attended = layer_call(z, factor, bias, gain, weight_all, *chains)
    return attended[None]


def solution(mesh):
    in_specs = (
        P(("grp", "dp"), "sp", None),
        P(("grp", "dp"), "sp"),
        P(None, "dp"),
        P(None, "dp"),
        P(None, "dp"),
        P(),
        P(),
        P(),
        P(),
    )
    out_specs = P(("grp", "dp"), "sp", None)
    return jax.shard_map(local, mesh=mesh, in_specs=in_specs, out_specs=out_specs, check_vma=False)
```

```python
import functools

import jax
import jax.numpy as jnp
from jax import lax
from jax.experimental import pallas as pl
from jax.experimental.pallas import tpu as pltpu
from jax.sharding import PartitionSpec as P

NEG = -1e30
QK_FLOOR = 0.1
OUT_FLOOR = 0.001
LOG2_E = 1.4426950408889634
PAD = 8
LAYER_VMEM = 60 << 20
BACKS = (7, 6)


NT = (((1,), (1,)), ((), ()))
VM = pl.BlockSpec(memory_space=pltpu.VMEM)
SM = pl.BlockSpec(memory_space=pltpu.SMEM)


def unit(vectors, axis):
    wide = vectors.astype(jnp.float32)
    mean = jnp.mean(wide * wide, axis=axis, keepdims=True)
    return wide * lax.rsqrt(mean + QK_FLOOR)


def pack_kernel(x_ref, gate_ref, shift_ref, bias_ref, first_ref, second_ref, wide_ref):
    half = second_ref.shape[0]
    rows = x_ref.shape[0]
    wide_ref[...] = jnp.broadcast_to(bias_ref[...], wide_ref.shape)
    first_ref[:half, :] = x_ref[:half, :]
    second_ref[...] = x_ref[half:, :]
    gates = lax.dot_general(gate_ref[...], x_ref[...], NT, preferred_element_type=jnp.float32)
    gates = (gates + shift_ref[...]).astype(jnp.bfloat16)
    first_ref[half:, :] = jnp.zeros((PAD, first_ref.shape[1]), jnp.bfloat16)
    for g in range(gates.shape[0] // PAD):
        first_ref[half:, g * rows : (g + 1) * rows] = gates[g * PAD : (g + 1) * PAD, :]


def bodies_of(n):
    bodies, k = [], 0
    while k < n:
        size = min(2 if k < 4 or k >= n - 4 else 4, n - k)
        bodies.append((k, size))
        k += size
    return bodies


def pairs_of(n):
    return [(k, first) for first, size in bodies_of(n) for k in range(first, first + size, 2)]


def load(firsts, seconds, x_of, x_sem, k, slot):
    half = seconds[0].shape[0]
    top, low = pl.ds(2 * slot * half, half), pl.ds((2 * slot + 1) * half, half)
    return (
        pltpu.make_async_copy(firsts[k].at[pl.ds(0, half), :], x_of.at[top], x_sem.at[slot, 0]),
        pltpu.make_async_copy(seconds[k], x_of.at[low], x_sem.at[slot, 1]),
    )


def keep(k_of, v_of, g, at, parts):
    piece = parts[0].shape[0] // 2
    keys = jnp.concatenate([part[:piece] for part in parts], axis=0)
    k_of[g, :, at] = unit(keys, 0).astype(jnp.bfloat16)
    v_of[g, :, at] = jnp.concatenate([part[piece:] for part in parts], axis=0)


def front_kernel(n, early, z_ref, weights_ref, *rest):
    count = 2 * len(early)
    firsts, seconds = rest[:count], rest[count : 2 * count]
    q_of, k_of, v_of, w_ref, x_of, w_sem, x_sem = rest[2 * count :]
    z = z_ref[0]
    rows = 2 * seconds[0].shape[0]
    heads, per_head, width = w_ref.shape
    groups, dim = k_of.shape[:2]
    group = heads // groups

    def fetch(h):
        return pltpu.make_async_copy(weights_ref.at[h], w_ref.at[h], w_sem.at[h])

    def copies(i):
        return load(firsts, seconds, x_of, x_sem, 2 * i, 2 * i) + load(
            firsts, seconds, x_of, x_sem, 2 * i + 1, 2 * i + 1
        )

    def start_pair(i):
        for copy in copies(i):
            copy.start()

    def own_pair(g, carry):
        for i in range(group):
            fetch(g * group + i).wait()
        made = lax.dot_general(
            w_ref[pl.ds(g * group, group)].reshape(group * per_head, width),
            x_of[: 2 * rows, :],
            NT,
            preferred_element_type=jnp.float32,
        ).astype(jnp.bfloat16)
        parts = []
        for i in range(group):
            at = i * per_head
            turned = unit(made[at : at + dim, :rows], 0).T
            q_of[g, i * rows : (i + 1) * rows, :] = turned.astype(jnp.bfloat16)
            parts.append(made[at + dim : at + per_head, :])
        keep(k_of, v_of, g, slice(0, 2 * rows), parts)
        return carry

    def other_pair(i, first):
        for copy in copies(i):
            copy.wait()
        made = lax.dot_general(
            w_ref[:, dim:, :].reshape(heads * (per_head - dim), width),
            x_of[2 * i * rows : (2 * i + 2) * rows, :],
            NT,
            preferred_element_type=jnp.float32,
        ).astype(jnp.bfloat16)
        size = per_head - dim
        parts = [made[h * size : (h + 1) * size] for h in range(heads)]
        for g in range(groups):
            at = slice(first * rows, (first + 2) * rows)
            keep(k_of, v_of, g, at, parts[g * group : (g + 1) * group])

    start_pair(0)
    for h in range(heads):
        fetch(h).start()
    for i, (_, body) in enumerate(early[1:], 1):
        pl.when(z >= body)(functools.partial(start_pair, i))
    for copy in copies(0):
        copy.wait()
    lax.fori_loop(0, groups, own_pair, 0)
    for i, (first, body) in enumerate(early[1:], 1):
        pl.when(z >= body)(functools.partial(other_pair, i, first))


def tail_kernel(n, late, z_ref, fac_ref, bias_ref, gain_ref, q_ref, k_ref, v_ref, w_all, *rest):
    firsts, seconds = rest[:n], rest[n : 2 * n]
    out_ref, q_of, k_of, v_of, bias_of, own_of, s_ref, m_ref, l_ref, acc_ref = rest[
        2 * n : 2 * n + 10
    ]
    w_ref, x_of, gates_of, w_sem, x_sem, gates_sem, q_sem, kv_sem = rest[2 * n + 10 :]
    z = z_ref[0]
    half = seconds[0].shape[0]
    rows = 2 * half
    heads, per_head, width = w_ref.shape
    groups, dim = k_of.shape[:2]
    group = heads // groups
    gate_rows = own_of.shape[0]
    bodies = bodies_of(n)

    def load_gates(k):
        return pltpu.make_async_copy(
            firsts[k].at[pl.ds(half, PAD), pl.ds(0, gates_of.shape[2])],
            gates_of.at[k],
            gates_sem.at[k],
        )

    queries = pltpu.make_async_copy(q_ref, q_of, q_sem)
    weights = pltpu.make_async_copy(w_all.at[:, pl.ds(dim, per_head), :], w_ref, w_sem)

    def made_before(i):
        first, size = bodies[i]
        at = pl.ds(first * rows, size * rows)
        return (
            pltpu.make_async_copy(k_ref.at[:, :, at], k_of.at[:, :, at], kv_sem.at[i, 0]),
            pltpu.make_async_copy(v_ref.at[:, :, at], v_of.at[:, :, at], kv_sem.at[i, 1]),
        )

    def start_all(copies):
        for copy in copies:
            copy.start()

    def wait_all(copies):
        for copy in copies:
            copy.wait()

    def late_copies(i, first):
        return load(firsts, seconds, x_of, x_sem, first, 2 * i) + load(
            firsts, seconds, x_of, x_sem, first + 1, 2 * i + 1
        )

    def late_pair(i, first):
        wait_all(late_copies(i, first))
        made = lax.dot_general(
            w_ref[...].reshape(heads * per_head, width),
            x_of[2 * i * rows : (2 * i + 2) * rows, :],
            NT,
            preferred_element_type=jnp.float32,
        ).astype(jnp.bfloat16)
        parts = [made[h * per_head : (h + 1) * per_head] for h in range(heads)]
        for g in range(groups):
            at = slice(first * rows, (first + 2) * rows)
            keep(k_of, v_of, g, at, parts[g * group : (g + 1) * group])

    for k in range(n):
        load_gates(k).start()
    queries.start()
    start_all(made_before(0))
    least = min(body for _, body in late)
    pl.when(z >= least)(weights.start)
    for i, (first, body) in enumerate(late):
        pl.when(z >= body)(functools.partial(start_all, late_copies(i, first)))
    for i, (first, _) in enumerate(bodies[1:], 1):
        pl.when(z >= first)(functools.partial(start_all, made_before(i)))
    for k in range(n):
        load_gates(k).wait()

    gates = [
        gates_of[k, :, g * rows : (g + 1) * rows].astype(jnp.float32)
        for k in range(n)
        for g in range(groups)
    ]
    gates = jnp.concatenate(gates, axis=0) + jnp.concatenate([bias_ref[...]] * n, axis=0)
    gates = jax.nn.log_sigmoid(gates) * LOG2_E
    lane = lax.broadcasted_iota(jnp.int32, gates.shape, 1)
    step = 1
    while step < rows:
        gates = gates + jnp.where(lane >= step, pltpu.roll(gates, step, 1), 0.0)
        step *= 2
    run = jnp.zeros((gate_rows, 1), jnp.float32)
    for k in range(n):
        gate = gates[k * gate_rows : (k + 1) * gate_rows, :]
        if k == 0:
            own_of[...] = gate
            bias_of[0] = -gate
        else:
            run = run + gate[:, rows - 1 :]
            bias_of[k] = jnp.where(z >= k, run - gate, NEG)

    queries.wait()
    wait_all(made_before(0))
    for i, (first, _) in enumerate(bodies[1:], 1):
        pl.when(z >= first)(functools.partial(wait_all, made_before(i)))
    pl.when(z >= least)(weights.wait)
    for i, (first, body) in enumerate(late):
        pl.when(z >= body)(functools.partial(late_pair, i, first))

    row = lax.broadcasted_iota(jnp.int32, (rows, rows), 0)
    col = lax.broadcasted_iota(jnp.int32, (rows, rows), 1)

    def one_group(g, carry):
        here = pl.ds(pl.multiple_of(g * PAD, PAD), PAD)
        own = own_of[here, :]
        columns = [
            jnp.sum(jnp.where(row == col, own[i : i + 1, :], 0.0), axis=1, keepdims=True)
            for i in range(group)
        ]

        def score(first, size):
            keys = k_of[g, :, first * rows : (first + size) * rows]
            dots = jnp.dot(q_of[g], keys, preferred_element_type=jnp.float32)
            biases = [bias_of[first + j, here, :] for j in range(size)]
            for i in range(group):
                mine = slice(i * rows, (i + 1) * rows)
                factor = fac_ref[g * group + i]
                most = None if first == 0 else m_ref[mine, :]
                for j in range(size):
                    part = dots[mine, j * rows : (j + 1) * rows] * factor
                    part = part + (columns[i] + biases[j][i : i + 1, :])
                    if first + j == 0:
                        part = jnp.where(col <= row, part, NEG)
                    s_ref[first + j, mine, :] = part
                    most = part if most is None else jnp.maximum(most, part)
                m_ref[mine, :] = most

        def mix(first, size):
            values = v_of[g, :, first * rows : (first + size) * rows]
            parts = []
            for i in range(group):
                mine = slice(i * rows, (i + 1) * rows)
                top = m_ref[mine, :]
                es = [jnp.exp2(s_ref[first + j, mine, :] - top) for j in range(size)]
                total = functools.reduce(jnp.add, es)
                parts.append(jnp.concatenate([e.astype(jnp.bfloat16) for e in es], axis=1))
                if first == 0:
                    l_ref[mine, :] = total
                else:
                    l_ref[mine, :] += total
            mixed = lax.dot_general(
                jnp.concatenate(parts, axis=0), values, NT, preferred_element_type=jnp.float32
            )
            if first == 0:
                acc_ref[...] = mixed
            else:
                acc_ref[...] += mixed

        score(*bodies[0])
        for first, size in bodies[1:]:
            pl.when(z >= first)(functools.partial(score, first, size))
        m_ref[...] = jnp.broadcast_to(jnp.max(m_ref[...], axis=1, keepdims=True), m_ref.shape)
        mix(*bodies[0])
        for first, size in bodies[1:]:
            pl.when(z >= first)(functools.partial(mix, first, size))
        for i in range(group):
            mine = slice(i * rows, (i + 1) * rows)
            mixed = acc_ref[mine, :] / jnp.sum(l_ref[mine, :], axis=1, keepdims=True)
            mean = jnp.mean(mixed * mixed, axis=-1, keepdims=True)
            head = pl.ds(pl.multiple_of((g * group + i) * dim, dim), dim)
            scaled = mixed * lax.rsqrt(mean + OUT_FLOOR) * gain_ref[:, head]
            out_ref[:, head] = scaled.astype(jnp.bfloat16)
        return carry

    lax.fori_loop(0, groups, one_group, 0)


def hbm(count):
    return [pl.BlockSpec(memory_space=pltpu.HBM)] * count


def front_call(z, weights, early, kv_heads, n, firsts, seconds):
    half, width = seconds[0].shape
    rows = 2 * half
    heads = weights.shape[0]
    dim = weights.shape[1] * heads // (heads + 2 * kv_heads)
    group = heads // kv_heads
    bf16 = jnp.bfloat16
    chosen = [k for first, _ in early for k in (first, first + 1)]
    turned = jax.ShapeDtypeStruct((kv_heads, dim, n * rows), bf16)
    return pl.pallas_call(
        functools.partial(front_kernel, n, early),
        in_specs=[SM] + hbm(1 + 2 * len(chosen)),
        out_specs=[VM] * 3,
        out_shape=[jax.ShapeDtypeStruct((kv_heads, group * rows, dim), bf16), turned, turned],
        scratch_shapes=[
            pltpu.VMEM(weights.shape, bf16),
            pltpu.VMEM((len(chosen) * rows, width), bf16),
            pltpu.SemaphoreType.DMA((heads,)),
            pltpu.SemaphoreType.DMA((len(chosen), 2)),
        ],
        cost_estimate=pl.CostEstimate(
            flops=2 * rows * n * width * heads * dim // 2,
            bytes_accessed=20 << 20,
            transcendentals=0,
        ),
        compiler_params=pltpu.CompilerParams(vmem_limit_bytes=LAYER_VMEM),
        name="front",
    )(z, weights, *[firsts[k] for k in chosen], *[seconds[k] for k in chosen])


def tail_call(z, factor, bias, gain, front, weights, late, firsts, seconds):
    half, width = seconds[0].shape
    rows = 2 * half
    n = len(firsts)
    gate_rows = bias.shape[0]
    kv_heads = gate_rows // PAD
    heads = weights.shape[0]
    dim = gain.shape[1] // heads
    group = heads // kv_heads
    bf16, f32 = jnp.bfloat16, jnp.float32
    return pl.pallas_call(
        functools.partial(tail_kernel, n, late),
        in_specs=[SM, SM, VM, VM] + hbm(4 + 2 * n),
        out_specs=VM,
        out_shape=jax.ShapeDtypeStruct((rows, heads * dim), bf16),
        scratch_shapes=[
            pltpu.VMEM((kv_heads, group * rows, dim), bf16),
            pltpu.VMEM((kv_heads, dim, n * rows), bf16),
            pltpu.VMEM((kv_heads, dim, n * rows), bf16),
            pltpu.VMEM((n, gate_rows, rows), f32),
            pltpu.VMEM((gate_rows, rows), f32),
            pltpu.VMEM((n, group * rows, rows), f32),
            pltpu.VMEM((group * rows, rows), f32),
            pltpu.VMEM((group * rows, rows), f32),
            pltpu.VMEM((group * rows, dim), f32),
            pltpu.VMEM((heads, weights.shape[1] - dim, width), bf16),
            pltpu.VMEM((2 * len(late) * rows, width), bf16),
            pltpu.VMEM((n, PAD, kv_heads * rows), bf16),
            pltpu.SemaphoreType.DMA,
            pltpu.SemaphoreType.DMA((2 * len(late), 2)),
            pltpu.SemaphoreType.DMA((n,)),
            pltpu.SemaphoreType.DMA,
            pltpu.SemaphoreType.DMA((len(bodies_of(n)), 2)),
        ],
        cost_estimate=pl.CostEstimate(
            flops=4 * rows * n * rows * heads * dim,
            bytes_accessed=12 << 20,
            transcendentals=1 << 22,
        ),
        compiler_params=pltpu.CompilerParams(vmem_limit_bytes=LAYER_VMEM),
        name="tail",
    )(z, factor, bias, gain, *front, weights, *firsts, *seconds)


def local(
    tokens,
    forget_offset,
    q_weight,
    k_weight,
    v_weight,
    forget_weight,
    forget_bias,
    score_gain,
    out_gain,
):
    x = tokens[0]
    rows, width = x.shape
    half = rows // 2
    heads = forget_bias.shape[0]
    dim = out_gain.shape[0] // heads
    n = lax.axis_size("sp")
    parts = lax.axis_size("dp")
    kv_heads = k_weight.shape[1] * parts // dim
    group = heads // kv_heads
    piece = 2 * k_weight.shape[1]
    z = lax.axis_index("sp").astype(jnp.int32).reshape(1)
    bf16, f32 = jnp.bfloat16, jnp.float32

    def padded(a):
        a = a.reshape(kv_heads, group, *a.shape[1:])
        return jnp.pad(a, ((0, 0), (0, PAD - group), (0, 0))).reshape(kv_heads * PAD, -1)

    gate_rows = kv_heads * PAD
    weight_own = jnp.concatenate([q_weight.T, k_weight.T, v_weight.T], axis=0)
    weight_all = lax.all_gather(weight_own, "dp", axis=0, tiled=False)

    *sent, bias = pl.pallas_call(
        pack_kernel,
        in_specs=[VM] * 4,
        out_specs=[VM] * 3,
        out_shape=[
            jax.ShapeDtypeStruct((half + PAD, width), bf16),
            jax.ShapeDtypeStruct((half, width), bf16),
            jax.ShapeDtypeStruct((gate_rows, rows), f32),
        ],
        cost_estimate=pl.CostEstimate(
            flops=2 * rows * width * gate_rows, bytes_accessed=1 << 20, transcendentals=0
        ),
        compiler_params=pltpu.CompilerParams(vmem_limit_bytes=16 << 20),
        name="pack",
    )(x, padded(forget_weight.T), forget_offset, padded(forget_bias[:, None]))

    sent, z, factor, bias, gain = lax.optimization_barrier(
        (
            sent,
            z,
            score_gain * (dim**-0.5 * LOG2_E),
            bias,
            out_gain[None, :],
        )
    )

    chains = [[block] + [None] * (n - 1) for block in sent]
    ups, downs = list(sent), list(sent)
    top = n - 1 - min(BACKS)
    late = [pair for pair in pairs_of(n) if pair[0] <= top < pair[0] + 2]
    early = [pair for pair in pairs_of(n) if pair not in late]
    front = None
    for k in range(1, top + 1):
        if k == top:
            front = front_call(z, weight_all, early, kv_heads, n, *chains)
            ups[1], front = lax.optimization_barrier((ups[1], front))
        rising = [(i, i + 1) for i in range(k - 1, n - 1)]
        for c, back in enumerate(BACKS):
            if k > n - 1 - back:
                continue
            if k <= back:
                sinking = [((b - k + 1) % n, (b - k) % n) for b in range(back)]
                down = lax.ppermute(downs[c], "sp", sinking)
            ups[c] = lax.ppermute(ups[c], "sp", rising)
            if k <= back:
                ups[c], downs[c] = lax.optimization_barrier((ups[c], down))
                chains[c][n - k] = downs[c]
            chains[c][k] = ups[c]

    attended = tail_call(z, factor, bias, gain, front, weight_all, late, *chains)
    return attended[None]


def solution(mesh):
    in_specs = (
        P(("grp", "dp"), "sp", None),
        P(("grp", "dp"), "sp"),
        P(None, "dp"),
        P(None, "dp"),
        P(None, "dp"),
        P(),
        P(),
        P(),
        P(),
    )
    out_specs = P(("grp", "dp"), "sp", None)
    return jax.shard_map(local, mesh=mesh, in_specs=in_specs, out_specs=out_specs, check_vma=False)
```

```python
import functools

import jax
import jax.numpy as jnp
from jax import lax
from jax.experimental import pallas as pl
from jax.experimental.pallas import tpu as pltpu
from jax.sharding import PartitionSpec as P

NEG = -1e30
QK_FLOOR = 0.1
OUT_FLOOR = 0.001
LOG2_E = 1.4426950408889634
PAD = 8
LAYER_VMEM = 60 << 20
BACKS = (7, 7)


NT = (((1,), (1,)), ((), ()))
VM = pl.BlockSpec(memory_space=pltpu.VMEM)
SM = pl.BlockSpec(memory_space=pltpu.SMEM)


def unit(vectors, axis):
    wide = vectors.astype(jnp.float32)
    mean = jnp.mean(wide * wide, axis=axis, keepdims=True)
    return wide * lax.rsqrt(mean + QK_FLOOR)


def pack_kernel(x_ref, gate_ref, shift_ref, bias_ref, first_ref, second_ref, wide_ref):
    half = second_ref.shape[0]
    rows = x_ref.shape[0]
    wide_ref[...] = jnp.broadcast_to(bias_ref[...], wide_ref.shape)
    first_ref[:half, :] = x_ref[:half, :]
    second_ref[...] = x_ref[half:, :]
    gates = lax.dot_general(gate_ref[...], x_ref[...], NT, preferred_element_type=jnp.float32)
    gates = (gates + shift_ref[...]).astype(jnp.bfloat16)
    first_ref[half:, :] = jnp.zeros((PAD, first_ref.shape[1]), jnp.bfloat16)
    for g in range(gates.shape[0] // PAD):
        first_ref[half:, g * rows : (g + 1) * rows] = gates[g * PAD : (g + 1) * PAD, :]


def bodies_of(n):
    bodies, k = [], 0
    while k < n:
        size = min(2 if k < 4 or k >= n - 4 else 4, n - k)
        bodies.append((k, size))
        k += size
    return bodies


def pairs_of(n):
    return [(k, first) for first, size in bodies_of(n) for k in range(first, first + size, 2)]


def load(firsts, seconds, x_of, x_sem, k, slot):
    half = seconds[0].shape[0]
    top, low = pl.ds(2 * slot * half, half), pl.ds((2 * slot + 1) * half, half)
    return (
        pltpu.make_async_copy(firsts[k].at[pl.ds(0, half), :], x_of.at[top], x_sem.at[slot, 0]),
        pltpu.make_async_copy(seconds[k], x_of.at[low], x_sem.at[slot, 1]),
    )


def keep(k_of, v_of, g, at, parts):
    piece = parts[0].shape[0] // 2
    keys = jnp.concatenate([part[:piece] for part in parts], axis=0)
    k_of[g, :, at] = unit(keys, 0).astype(jnp.bfloat16)
    v_of[g, :, at] = jnp.concatenate([part[piece:] for part in parts], axis=0)


def front_kernel(n, early, z_ref, weights_ref, *rest):
    count = 2 * len(early)
    firsts, seconds = rest[:count], rest[count : 2 * count]
    q_of, k_of, v_of, w_ref, x_of, w_sem, x_sem = rest[2 * count :]
    z = z_ref[0]
    rows = 2 * seconds[0].shape[0]
    heads, per_head, width = w_ref.shape
    groups, dim = k_of.shape[:2]
    group = heads // groups

    def fetch(h):
        return pltpu.make_async_copy(weights_ref.at[h], w_ref.at[h], w_sem.at[h])

    def copies(i):
        return load(firsts, seconds, x_of, x_sem, 2 * i, 2 * i) + load(
            firsts, seconds, x_of, x_sem, 2 * i + 1, 2 * i + 1
        )

    def start_pair(i):
        for copy in copies(i):
            copy.start()

    def own_pair(g, carry):
        for i in range(group):
            fetch(g * group + i).wait()
        made = lax.dot_general(
            w_ref[pl.ds(g * group, group)].reshape(group * per_head, width),
            x_of[: 2 * rows, :],
            NT,
            preferred_element_type=jnp.float32,
        ).astype(jnp.bfloat16)
        parts = []
        for i in range(group):
            at = i * per_head
            turned = unit(made[at : at + dim, :rows], 0).T
            q_of[g, i * rows : (i + 1) * rows, :] = turned.astype(jnp.bfloat16)
            parts.append(made[at + dim : at + per_head, :])
        keep(k_of, v_of, g, slice(0, 2 * rows), parts)
        return carry

    def other_pair(i, first):
        for copy in copies(i):
            copy.wait()
        made = lax.dot_general(
            w_ref[:, dim:, :].reshape(heads * (per_head - dim), width),
            x_of[2 * i * rows : (2 * i + 2) * rows, :],
            NT,
            preferred_element_type=jnp.float32,
        ).astype(jnp.bfloat16)
        size = per_head - dim
        parts = [made[h * size : (h + 1) * size] for h in range(heads)]
        for g in range(groups):
            at = slice(first * rows, (first + 2) * rows)
            keep(k_of, v_of, g, at, parts[g * group : (g + 1) * group])

    start_pair(0)
    for h in range(heads):
        fetch(h).start()
    for i, (_, body) in enumerate(early[1:], 1):
        pl.when(z >= body)(functools.partial(start_pair, i))
    for copy in copies(0):
        copy.wait()
    lax.fori_loop(0, groups, own_pair, 0)
    for i, (first, body) in enumerate(early[1:], 1):
        pl.when(z >= body)(functools.partial(other_pair, i, first))


def tail_kernel(n, late, z_ref, fac_ref, bias_ref, gain_ref, q_ref, k_ref, v_ref, w_all, *rest):
    firsts, seconds = rest[:n], rest[n : 2 * n]
    out_ref, q_of, k_of, v_of, bias_of, own_of, s_ref, m_ref, l_ref, acc_ref = rest[
        2 * n : 2 * n + 10
    ]
    w_ref, x_of, gates_of, w_sem, x_sem, gates_sem, q_sem, kv_sem = rest[2 * n + 10 :]
    z = z_ref[0]
    half = seconds[0].shape[0]
    rows = 2 * half
    heads, per_head, width = w_ref.shape
    groups, dim = k_of.shape[:2]
    group = heads // groups
    gate_rows = own_of.shape[0]
    bodies = bodies_of(n)

    def load_gates(k):
        return pltpu.make_async_copy(
            firsts[k].at[pl.ds(half, PAD), pl.ds(0, gates_of.shape[2])],
            gates_of.at[k],
            gates_sem.at[k],
        )

    queries = pltpu.make_async_copy(q_ref, q_of, q_sem)
    weights = [
        pltpu.make_async_copy(w_all.at[h, pl.ds(dim, per_head), :], w_ref.at[h], w_sem.at[h])
        for h in range(heads)
    ]

    def made_before(i):
        first, size = bodies[i]
        at = pl.ds(first * rows, size * rows)
        return (
            pltpu.make_async_copy(k_ref.at[:, :, at], k_of.at[:, :, at], kv_sem.at[i, 0]),
            pltpu.make_async_copy(v_ref.at[:, :, at], v_of.at[:, :, at], kv_sem.at[i, 1]),
        )

    def start_all(copies):
        for copy in copies:
            copy.start()

    def wait_all(copies):
        for copy in copies:
            copy.wait()

    def late_copies(i, first):
        return load(firsts, seconds, x_of, x_sem, first, 2 * i) + load(
            firsts, seconds, x_of, x_sem, first + 1, 2 * i + 1
        )

    def late_pair(i, first):
        wait_all(late_copies(i, first))
        made = lax.dot_general(
            w_ref[...].reshape(heads * per_head, width),
            x_of[2 * i * rows : (2 * i + 2) * rows, :],
            NT,
            preferred_element_type=jnp.float32,
        ).astype(jnp.bfloat16)
        parts = [made[h * per_head : (h + 1) * per_head] for h in range(heads)]
        for g in range(groups):
            at = slice(first * rows, (first + 2) * rows)
            keep(k_of, v_of, g, at, parts[g * group : (g + 1) * group])

    for k in range(n):
        load_gates(k).start()
    queries.start()
    start_all(made_before(0))
    least = min(body for _, body in late)
    pl.when(z >= least)(functools.partial(start_all, weights))
    for i, (first, body) in enumerate(late):
        pl.when(z >= body)(functools.partial(start_all, late_copies(i, first)))
    for i, (first, _) in enumerate(bodies[1:], 1):
        pl.when(z >= first)(functools.partial(start_all, made_before(i)))
    for k in range(n):
        load_gates(k).wait()

    gates = [
        gates_of[k, :, g * rows : (g + 1) * rows].astype(jnp.float32)
        for k in range(n)
        for g in range(groups)
    ]
    gates = jnp.concatenate(gates, axis=0) + jnp.concatenate([bias_ref[...]] * n, axis=0)
    gates = jax.nn.log_sigmoid(gates) * LOG2_E
    lane = lax.broadcasted_iota(jnp.int32, gates.shape, 1)
    step = 1
    while step < rows:
        gates = gates + jnp.where(lane >= step, pltpu.roll(gates, step, 1), 0.0)
        step *= 2
    run = jnp.zeros((gate_rows, 1), jnp.float32)
    for k in range(n):
        gate = gates[k * gate_rows : (k + 1) * gate_rows, :]
        if k == 0:
            own_of[...] = gate
            bias_of[0] = -gate
        else:
            run = run + gate[:, rows - 1 :]
            bias_of[k] = jnp.where(z >= k, run - gate, NEG)

    queries.wait()
    wait_all(made_before(0))
    for i, (first, _) in enumerate(bodies[1:], 1):
        pl.when(z >= first)(functools.partial(wait_all, made_before(i)))
    pl.when(z >= least)(functools.partial(wait_all, weights))
    for i, (first, body) in enumerate(late):
        pl.when(z >= body)(functools.partial(late_pair, i, first))

    row = lax.broadcasted_iota(jnp.int32, (rows, rows), 0)
    col = lax.broadcasted_iota(jnp.int32, (rows, rows), 1)

    def one_group(g, carry):
        here = pl.ds(pl.multiple_of(g * PAD, PAD), PAD)
        own = own_of[here, :]
        columns = [
            jnp.sum(jnp.where(row == col, own[i : i + 1, :], 0.0), axis=1, keepdims=True)
            for i in range(group)
        ]

        def score(first, size):
            keys = k_of[g, :, first * rows : (first + size) * rows]
            dots = jnp.dot(q_of[g], keys, preferred_element_type=jnp.float32)
            biases = [bias_of[first + j, here, :] for j in range(size)]
            for i in range(group):
                mine = slice(i * rows, (i + 1) * rows)
                factor = fac_ref[g * group + i]
                most = None if first == 0 else m_ref[mine, :]
                for j in range(size):
                    part = dots[mine, j * rows : (j + 1) * rows] * factor
                    part = part + (columns[i] + biases[j][i : i + 1, :])
                    if first + j == 0:
                        part = jnp.where(col <= row, part, NEG)
                    s_ref[first + j, mine, :] = part
                    most = part if most is None else jnp.maximum(most, part)
                m_ref[mine, :] = most

        def mix(first, size):
            values = v_of[g, :, first * rows : (first + size) * rows]
            parts = []
            for i in range(group):
                mine = slice(i * rows, (i + 1) * rows)
                top = m_ref[mine, :]
                es = [jnp.exp2(s_ref[first + j, mine, :] - top) for j in range(size)]
                total = functools.reduce(jnp.add, es)
                parts.append(jnp.concatenate([e.astype(jnp.bfloat16) for e in es], axis=1))
                if first == 0:
                    l_ref[mine, :] = total
                else:
                    l_ref[mine, :] += total
            mixed = lax.dot_general(
                jnp.concatenate(parts, axis=0), values, NT, preferred_element_type=jnp.float32
            )
            if first == 0:
                acc_ref[...] = mixed
            else:
                acc_ref[...] += mixed

        score(*bodies[0])
        for first, size in bodies[1:]:
            pl.when(z >= first)(functools.partial(score, first, size))
        m_ref[...] = jnp.broadcast_to(jnp.max(m_ref[...], axis=1, keepdims=True), m_ref.shape)
        mix(*bodies[0])
        for first, size in bodies[1:]:
            pl.when(z >= first)(functools.partial(mix, first, size))
        for i in range(group):
            mine = slice(i * rows, (i + 1) * rows)
            mixed = acc_ref[mine, :] / jnp.sum(l_ref[mine, :], axis=1, keepdims=True)
            mean = jnp.mean(mixed * mixed, axis=-1, keepdims=True)
            head = pl.ds(pl.multiple_of((g * group + i) * dim, dim), dim)
            scaled = mixed * lax.rsqrt(mean + OUT_FLOOR) * gain_ref[:, head]
            out_ref[:, head] = scaled.astype(jnp.bfloat16)
        return carry

    lax.fori_loop(0, groups, one_group, 0)


def hbm(count):
    return [pl.BlockSpec(memory_space=pltpu.HBM)] * count


def front_call(z, weights, early, kv_heads, n, firsts, seconds):
    half, width = seconds[0].shape
    rows = 2 * half
    heads = weights.shape[0]
    dim = weights.shape[1] * heads // (heads + 2 * kv_heads)
    group = heads // kv_heads
    bf16 = jnp.bfloat16
    chosen = [k for first, _ in early for k in (first, first + 1)]
    turned = jax.ShapeDtypeStruct((kv_heads, dim, n * rows), bf16)
    return pl.pallas_call(
        functools.partial(front_kernel, n, early),
        in_specs=[SM] + hbm(1 + 2 * len(chosen)),
        out_specs=[VM] * 3,
        out_shape=[jax.ShapeDtypeStruct((kv_heads, group * rows, dim), bf16), turned, turned],
        scratch_shapes=[
            pltpu.VMEM(weights.shape, bf16),
            pltpu.VMEM((len(chosen) * rows, width), bf16),
            pltpu.SemaphoreType.DMA((heads,)),
            pltpu.SemaphoreType.DMA((len(chosen), 2)),
        ],
        cost_estimate=pl.CostEstimate(
            flops=2 * rows * n * width * heads * dim // 2,
            bytes_accessed=20 << 20,
            transcendentals=0,
        ),
        compiler_params=pltpu.CompilerParams(vmem_limit_bytes=LAYER_VMEM),
        name="front",
    )(z, weights, *[firsts[k] for k in chosen], *[seconds[k] for k in chosen])


def tail_call(z, factor, bias, gain, front, weights, late, firsts, seconds):
    half, width = seconds[0].shape
    rows = 2 * half
    n = len(firsts)
    gate_rows = bias.shape[0]
    kv_heads = gate_rows // PAD
    heads = weights.shape[0]
    dim = gain.shape[1] // heads
    group = heads // kv_heads
    bf16, f32 = jnp.bfloat16, jnp.float32
    return pl.pallas_call(
        functools.partial(tail_kernel, n, late),
        in_specs=[SM, SM, VM, VM] + hbm(4 + 2 * n),
        out_specs=VM,
        out_shape=jax.ShapeDtypeStruct((rows, heads * dim), bf16),
        scratch_shapes=[
            pltpu.VMEM((kv_heads, group * rows, dim), bf16),
            pltpu.VMEM((kv_heads, dim, n * rows), bf16),
            pltpu.VMEM((kv_heads, dim, n * rows), bf16),
            pltpu.VMEM((n, gate_rows, rows), f32),
            pltpu.VMEM((gate_rows, rows), f32),
            pltpu.VMEM((n, group * rows, rows), f32),
            pltpu.VMEM((group * rows, rows), f32),
            pltpu.VMEM((group * rows, rows), f32),
            pltpu.VMEM((group * rows, dim), f32),
            pltpu.VMEM((heads, weights.shape[1] - dim, width), bf16),
            pltpu.VMEM((2 * len(late) * rows, width), bf16),
            pltpu.VMEM((n, PAD, kv_heads * rows), bf16),
            pltpu.SemaphoreType.DMA((heads,)),
            pltpu.SemaphoreType.DMA((2 * len(late), 2)),
            pltpu.SemaphoreType.DMA((n,)),
            pltpu.SemaphoreType.DMA,
            pltpu.SemaphoreType.DMA((len(bodies_of(n)), 2)),
        ],
        cost_estimate=pl.CostEstimate(
            flops=4 * rows * n * rows * heads * dim,
            bytes_accessed=12 << 20,
            transcendentals=1 << 22,
        ),
        compiler_params=pltpu.CompilerParams(vmem_limit_bytes=LAYER_VMEM),
        name="tail",
    )(z, factor, bias, gain, *front, weights, *firsts, *seconds)


def local(
    tokens,
    forget_offset,
    q_weight,
    k_weight,
    v_weight,
    forget_weight,
    forget_bias,
    score_gain,
    out_gain,
):
    x = tokens[0]
    rows, width = x.shape
    half = rows // 2
    heads = forget_bias.shape[0]
    dim = out_gain.shape[0] // heads
    n = lax.axis_size("sp")
    parts = lax.axis_size("dp")
    kv_heads = k_weight.shape[1] * parts // dim
    group = heads // kv_heads
    piece = 2 * k_weight.shape[1]
    z = lax.axis_index("sp").astype(jnp.int32).reshape(1)
    bf16, f32 = jnp.bfloat16, jnp.float32

    def padded(a):
        a = a.reshape(kv_heads, group, *a.shape[1:])
        return jnp.pad(a, ((0, 0), (0, PAD - group), (0, 0))).reshape(kv_heads * PAD, -1)

    gate_rows = kv_heads * PAD
    weight_own = jnp.concatenate([q_weight.T, k_weight.T, v_weight.T], axis=0)
    weight_all = lax.all_gather(weight_own, "dp", axis=0, tiled=False)

    *sent, bias = pl.pallas_call(
        pack_kernel,
        in_specs=[VM] * 4,
        out_specs=[VM] * 3,
        out_shape=[
            jax.ShapeDtypeStruct((half + PAD, width), bf16),
            jax.ShapeDtypeStruct((half, width), bf16),
            jax.ShapeDtypeStruct((gate_rows, rows), f32),
        ],
        cost_estimate=pl.CostEstimate(
            flops=2 * rows * width * gate_rows, bytes_accessed=1 << 20, transcendentals=0
        ),
        compiler_params=pltpu.CompilerParams(vmem_limit_bytes=16 << 20),
        name="pack",
    )(x, padded(forget_weight.T), forget_offset, padded(forget_bias[:, None]))

    sent, z, factor, bias, gain = lax.optimization_barrier(
        (
            sent,
            z,
            score_gain * (dim**-0.5 * LOG2_E),
            bias,
            out_gain[None, :],
        )
    )

    chains = [[block] + [None] * (n - 1) for block in sent]
    ups, downs = list(sent), list(sent)
    top = n - 1 - min(BACKS)
    late = [pair for pair in pairs_of(n) if pair[0] <= top < pair[0] + 2]
    early = [pair for pair in pairs_of(n) if pair not in late]
    for k in range(1, top + 1):
        rising = [(i, i + 1) for i in range(k - 1, n - 1)]
        for c, back in enumerate(BACKS):
            if k > n - 1 - back:
                continue
            if k <= back:
                sinking = [((b - k + 1) % n, (b - k) % n) for b in range(back)]
                down = lax.ppermute(downs[c], "sp", sinking)
            ups[c] = lax.ppermute(ups[c], "sp", rising)
            if k <= back:
                ups[c], downs[c] = lax.optimization_barrier((ups[c], down))
                chains[c][n - k] = downs[c]
            chains[c][k] = ups[c]

    front = front_call(z, weight_all, early, kv_heads, n, *chains)
    attended = tail_call(z, factor, bias, gain, front, weight_all, late, *chains)
    return attended[None]


def solution(mesh):
    in_specs = (
        P(("grp", "dp"), "sp", None),
        P(("grp", "dp"), "sp"),
        P(None, "dp"),
        P(None, "dp"),
        P(None, "dp"),
        P(),
        P(),
        P(),
        P(),
    )
    out_specs = P(("grp", "dp"), "sp", None)
    return jax.shard_map(local, mesh=mesh, in_specs=in_specs, out_specs=out_specs, check_vma=False)
```

```python
import functools

import jax
import jax.numpy as jnp
from jax import lax
from jax.experimental import pallas as pl
from jax.experimental.pallas import tpu as pltpu
from jax.sharding import PartitionSpec as P

NEG = -1e30
QK_FLOOR = 0.1
OUT_FLOOR = 0.001
LOG2_E = 1.4426950408889634
PAD = 8
LAYER_VMEM = 60 << 20
BACKS = (7, 7)


NT = (((1,), (1,)), ((), ()))
VM = pl.BlockSpec(memory_space=pltpu.VMEM)
SM = pl.BlockSpec(memory_space=pltpu.SMEM)


def unit(vectors, axis):
    wide = vectors.astype(jnp.float32)
    mean = jnp.mean(wide * wide, axis=axis, keepdims=True)
    return wide * lax.rsqrt(mean + QK_FLOOR)


def pack_kernel(
    x_ref, gate_ref, shift_ref, bias_ref, q_ref, k_ref, v_ref, first_ref, second_ref, wide_ref, own_ref
):
    half = second_ref.shape[0]
    rows = x_ref.shape[0]
    wide_ref[...] = jnp.broadcast_to(bias_ref[...], wide_ref.shape)
    dim, piece = q_ref.shape[1], k_ref.shape[0]
    own_ref[:dim, :] = q_ref[...].astype(jnp.float32).T.astype(jnp.bfloat16)
    own_ref[dim : dim + piece, :] = k_ref[...]
    own_ref[dim + piece :, :] = v_ref[...]
    first_ref[:half, :] = x_ref[:half, :]
    second_ref[...] = x_ref[half:, :]
    gates = lax.dot_general(gate_ref[...], x_ref[...], NT, preferred_element_type=jnp.float32)
    gates = (gates + shift_ref[...]).astype(jnp.bfloat16)
    first_ref[half:, :] = jnp.zeros((PAD, first_ref.shape[1]), jnp.bfloat16)
    for g in range(gates.shape[0] // PAD):
        first_ref[half:, g * rows : (g + 1) * rows] = gates[g * PAD : (g + 1) * PAD, :]


def bodies_of(n):
    bodies, k = [], 0
    while k < n:
        size = min(2 if k < 4 or k >= n - 4 else 4, n - k)
        bodies.append((k, size))
        k += size
    return bodies


def pairs_of(n):
    return [(k, first) for first, size in bodies_of(n) for k in range(first, first + size, 2)]


def load(firsts, seconds, x_of, x_sem, k, slot):
    half = seconds[0].shape[0]
    top, low = pl.ds(2 * slot * half, half), pl.ds((2 * slot + 1) * half, half)
    return (
        pltpu.make_async_copy(firsts[k].at[pl.ds(0, half), :], x_of.at[top], x_sem.at[slot, 0]),
        pltpu.make_async_copy(seconds[k], x_of.at[low], x_sem.at[slot, 1]),
    )


def keep(k_of, v_of, g, at, parts):
    piece = parts[0].shape[0] // 2
    keys = jnp.concatenate([part[:piece] for part in parts], axis=0)
    k_of[g, :, at] = unit(keys, 0).astype(jnp.bfloat16)
    v_of[g, :, at] = jnp.concatenate([part[piece:] for part in parts], axis=0)


def front_kernel(n, early, z_ref, weights_ref, *rest):
    count = 2 * len(early)
    firsts, seconds = rest[:count], rest[count : 2 * count]
    q_of, k_of, v_of, w_ref, x_of, w_sem, x_sem = rest[2 * count :]
    z = z_ref[0]
    rows = 2 * seconds[0].shape[0]
    heads, per_head, width = w_ref.shape
    groups, dim = k_of.shape[:2]
    group = heads // groups

    def fetch(h):
        return pltpu.make_async_copy(weights_ref.at[h], w_ref.at[h], w_sem.at[h])

    def copies(i):
        return load(firsts, seconds, x_of, x_sem, 2 * i, 2 * i) + load(
            firsts, seconds, x_of, x_sem, 2 * i + 1, 2 * i + 1
        )

    def start_pair(i):
        for copy in copies(i):
            copy.start()

    def own_pair(g, carry):
        for i in range(group):
            fetch(g * group + i).wait()
        made = lax.dot_general(
            w_ref[pl.ds(g * group, group)].reshape(group * per_head, width),
            x_of[: 2 * rows, :],
            NT,
            preferred_element_type=jnp.float32,
        ).astype(jnp.bfloat16)
        parts = []
        for i in range(group):
            at = i * per_head
            turned = unit(made[at : at + dim, :rows], 0).T
            q_of[g, i * rows : (i + 1) * rows, :] = turned.astype(jnp.bfloat16)
            parts.append(made[at + dim : at + per_head, :])
        keep(k_of, v_of, g, slice(0, 2 * rows), parts)
        return carry

    def other_pair(i, first):
        for copy in copies(i):
            copy.wait()
        made = lax.dot_general(
            w_ref[:, dim:, :].reshape(heads * (per_head - dim), width),
            x_of[2 * i * rows : (2 * i + 2) * rows, :],
            NT,
            preferred_element_type=jnp.float32,
        ).astype(jnp.bfloat16)
        size = per_head - dim
        parts = [made[h * size : (h + 1) * size] for h in range(heads)]
        for g in range(groups):
            at = slice(first * rows, (first + 2) * rows)
            keep(k_of, v_of, g, at, parts[g * group : (g + 1) * group])

    start_pair(0)
    for h in range(heads):
        fetch(h).start()
    for i, (_, body) in enumerate(early[1:], 1):
        pl.when(z >= body)(functools.partial(start_pair, i))
    for copy in copies(0):
        copy.wait()
    lax.fori_loop(0, groups, own_pair, 0)
    for i, (first, body) in enumerate(early[1:], 1):
        pl.when(z >= body)(functools.partial(other_pair, i, first))


def tail_kernel(n, late, z_ref, fac_ref, bias_ref, gain_ref, q_ref, k_ref, v_ref, w_all, *rest):
    firsts, seconds = rest[:n], rest[n : 2 * n]
    out_ref, q_of, k_of, v_of, bias_of, own_of, s_ref, m_ref, l_ref, acc_ref = rest[
        2 * n : 2 * n + 10
    ]
    w_ref, x_of, gates_of, w_sem, x_sem, gates_sem, q_sem, kv_sem = rest[2 * n + 10 :]
    z = z_ref[0]
    half = seconds[0].shape[0]
    rows = 2 * half
    heads, per_head, width = w_ref.shape
    groups, dim = k_of.shape[:2]
    group = heads // groups
    gate_rows = own_of.shape[0]
    bodies = bodies_of(n)

    def load_gates(k):
        return pltpu.make_async_copy(
            firsts[k].at[pl.ds(half, PAD), pl.ds(0, gates_of.shape[2])],
            gates_of.at[k],
            gates_sem.at[k],
        )

    queries = pltpu.make_async_copy(q_ref, q_of, q_sem)
    weights = [
        pltpu.make_async_copy(w_all.at[h, pl.ds(dim, per_head), :], w_ref.at[h], w_sem.at[h])
        for h in range(heads)
    ]

    def made_before(i):
        first, size = bodies[i]
        at = pl.ds(first * rows, size * rows)
        return (
            pltpu.make_async_copy(k_ref.at[:, :, at], k_of.at[:, :, at], kv_sem.at[i, 0]),
            pltpu.make_async_copy(v_ref.at[:, :, at], v_of.at[:, :, at], kv_sem.at[i, 1]),
        )

    def start_all(copies):
        for copy in copies:
            copy.start()

    def wait_all(copies):
        for copy in copies:
            copy.wait()

    def late_copies(i, first):
        return load(firsts, seconds, x_of, x_sem, first, 2 * i) + load(
            firsts, seconds, x_of, x_sem, first + 1, 2 * i + 1
        )

    def late_pair(i, first):
        wait_all(late_copies(i, first))
        made = lax.dot_general(
            w_ref[...].reshape(heads * per_head, width),
            x_of[2 * i * rows : (2 * i + 2) * rows, :],
            NT,
            preferred_element_type=jnp.float32,
        ).astype(jnp.bfloat16)
        parts = [made[h * per_head : (h + 1) * per_head] for h in range(heads)]
        for g in range(groups):
            at = slice(first * rows, (first + 2) * rows)
            keep(k_of, v_of, g, at, parts[g * group : (g + 1) * group])

    for k in range(n):
        load_gates(k).start()
    queries.start()
    start_all(made_before(0))
    least = min(body for _, body in late)
    pl.when(z >= least)(functools.partial(start_all, weights))
    for i, (first, body) in enumerate(late):
        pl.when(z >= body)(functools.partial(start_all, late_copies(i, first)))
    for i, (first, _) in enumerate(bodies[1:], 1):
        pl.when(z >= first)(functools.partial(start_all, made_before(i)))
    for k in range(n):
        load_gates(k).wait()

    gates = [
        gates_of[k, :, g * rows : (g + 1) * rows].astype(jnp.float32)
        for k in range(n)
        for g in range(groups)
    ]
    gates = jnp.concatenate(gates, axis=0) + jnp.concatenate([bias_ref[...]] * n, axis=0)
    gates = jax.nn.log_sigmoid(gates) * LOG2_E
    lane = lax.broadcasted_iota(jnp.int32, gates.shape, 1)
    step = 1
    while step < rows:
        gates = gates + jnp.where(lane >= step, pltpu.roll(gates, step, 1), 0.0)
        step *= 2
    run = jnp.zeros((gate_rows, 1), jnp.float32)
    for k in range(n):
        gate = gates[k * gate_rows : (k + 1) * gate_rows, :]
        if k == 0:
            own_of[...] = gate
            bias_of[0] = -gate
        else:
            run = run + gate[:, rows - 1 :]
            bias_of[k] = jnp.where(z >= k, run - gate, NEG)

    queries.wait()
    wait_all(made_before(0))
    for i, (first, _) in enumerate(bodies[1:], 1):
        pl.when(z >= first)(functools.partial(wait_all, made_before(i)))
    pl.when(z >= least)(functools.partial(wait_all, weights))
    for i, (first, body) in enumerate(late):
        pl.when(z >= body)(functools.partial(late_pair, i, first))

    row = lax.broadcasted_iota(jnp.int32, (rows, rows), 0)
    col = lax.broadcasted_iota(jnp.int32, (rows, rows), 1)

    def one_group(g, carry):
        here = pl.ds(pl.multiple_of(g * PAD, PAD), PAD)
        own = own_of[here, :]
        columns = [
            jnp.sum(jnp.where(row == col, own[i : i + 1, :], 0.0), axis=1, keepdims=True)
            for i in range(group)
        ]

        def score(first, size):
            keys = k_of[g, :, first * rows : (first + size) * rows]
            dots = jnp.dot(q_of[g], keys, preferred_element_type=jnp.float32)
            biases = [bias_of[first + j, here, :] for j in range(size)]
            for i in range(group):
                mine = slice(i * rows, (i + 1) * rows)
                factor = fac_ref[g * group + i]
                most = None if first == 0 else m_ref[mine, :]
                for j in range(size):
                    part = dots[mine, j * rows : (j + 1) * rows] * factor
                    part = part + (columns[i] + biases[j][i : i + 1, :])
                    if first + j == 0:
                        part = jnp.where(col <= row, part, NEG)
                    s_ref[first + j, mine, :] = part
                    most = part if most is None else jnp.maximum(most, part)
                m_ref[mine, :] = most

        def mix(first, size):
            values = v_of[g, :, first * rows : (first + size) * rows]
            parts = []
            for i in range(group):
                mine = slice(i * rows, (i + 1) * rows)
                top = m_ref[mine, :]
                es = [jnp.exp2(s_ref[first + j, mine, :] - top) for j in range(size)]
                total = functools.reduce(jnp.add, es)
                parts.append(jnp.concatenate([e.astype(jnp.bfloat16) for e in es], axis=1))
                if first == 0:
                    l_ref[mine, :] = total
                else:
                    l_ref[mine, :] += total
            mixed = lax.dot_general(
                jnp.concatenate(parts, axis=0), values, NT, preferred_element_type=jnp.float32
            )
            if first == 0:
                acc_ref[...] = mixed
            else:
                acc_ref[...] += mixed

        score(*bodies[0])
        for first, size in bodies[1:]:
            pl.when(z >= first)(functools.partial(score, first, size))
        m_ref[...] = jnp.broadcast_to(jnp.max(m_ref[...], axis=1, keepdims=True), m_ref.shape)
        mix(*bodies[0])
        for first, size in bodies[1:]:
            pl.when(z >= first)(functools.partial(mix, first, size))
        for i in range(group):
            mine = slice(i * rows, (i + 1) * rows)
            mixed = acc_ref[mine, :] / jnp.sum(l_ref[mine, :], axis=1, keepdims=True)
            mean = jnp.mean(mixed * mixed, axis=-1, keepdims=True)
            head = pl.ds(pl.multiple_of((g * group + i) * dim, dim), dim)
            scaled = mixed * lax.rsqrt(mean + OUT_FLOOR) * gain_ref[:, head]
            out_ref[:, head] = scaled.astype(jnp.bfloat16)
        return carry

    lax.fori_loop(0, groups, one_group, 0)


def hbm(count):
    return [pl.BlockSpec(memory_space=pltpu.HBM)] * count


def front_call(z, weights, early, kv_heads, n, firsts, seconds):
    half, width = seconds[0].shape
    rows = 2 * half
    heads = weights.shape[0]
    dim = weights.shape[1] * heads // (heads + 2 * kv_heads)
    group = heads // kv_heads
    bf16 = jnp.bfloat16
    chosen = [k for first, _ in early for k in (first, first + 1)]
    turned = jax.ShapeDtypeStruct((kv_heads, dim, n * rows), bf16)
    return pl.pallas_call(
        functools.partial(front_kernel, n, early),
        in_specs=[SM] + hbm(1 + 2 * len(chosen)),
        out_specs=[VM] * 3,
        out_shape=[jax.ShapeDtypeStruct((kv_heads, group * rows, dim), bf16), turned, turned],
        scratch_shapes=[
            pltpu.VMEM(weights.shape, bf16),
            pltpu.VMEM((len(chosen) * rows, width), bf16),
            pltpu.SemaphoreType.DMA((heads,)),
            pltpu.SemaphoreType.DMA((len(chosen), 2)),
        ],
        cost_estimate=pl.CostEstimate(
            flops=2 * rows * n * width * heads * dim // 2,
            bytes_accessed=20 << 20,
            transcendentals=0,
        ),
        compiler_params=pltpu.CompilerParams(vmem_limit_bytes=LAYER_VMEM),
        name="front",
    )(z, weights, *[firsts[k] for k in chosen], *[seconds[k] for k in chosen])


def tail_call(z, factor, bias, gain, front, weights, late, firsts, seconds):
    half, width = seconds[0].shape
    rows = 2 * half
    n = len(firsts)
    gate_rows = bias.shape[0]
    kv_heads = gate_rows // PAD
    heads = weights.shape[0]
    dim = gain.shape[1] // heads
    group = heads // kv_heads
    bf16, f32 = jnp.bfloat16, jnp.float32
    return pl.pallas_call(
        functools.partial(tail_kernel, n, late),
        in_specs=[SM, SM, VM, VM] + hbm(4 + 2 * n),
        out_specs=VM,
        out_shape=jax.ShapeDtypeStruct((rows, heads * dim), bf16),
        scratch_shapes=[
            pltpu.VMEM((kv_heads, group * rows, dim), bf16),
            pltpu.VMEM((kv_heads, dim, n * rows), bf16),
            pltpu.VMEM((kv_heads, dim, n * rows), bf16),
            pltpu.VMEM((n, gate_rows, rows), f32),
            pltpu.VMEM((gate_rows, rows), f32),
            pltpu.VMEM((n, group * rows, rows), f32),
            pltpu.VMEM((group * rows, rows), f32),
            pltpu.VMEM((group * rows, rows), f32),
            pltpu.VMEM((group * rows, dim), f32),
            pltpu.VMEM((heads, weights.shape[1] - dim, width), bf16),
            pltpu.VMEM((2 * len(late) * rows, width), bf16),
            pltpu.VMEM((n, PAD, kv_heads * rows), bf16),
            pltpu.SemaphoreType.DMA((heads,)),
            pltpu.SemaphoreType.DMA((2 * len(late), 2)),
            pltpu.SemaphoreType.DMA((n,)),
            pltpu.SemaphoreType.DMA,
            pltpu.SemaphoreType.DMA((len(bodies_of(n)), 2)),
        ],
        cost_estimate=pl.CostEstimate(
            flops=4 * rows * n * rows * heads * dim,
            bytes_accessed=12 << 20,
            transcendentals=1 << 22,
        ),
        compiler_params=pltpu.CompilerParams(vmem_limit_bytes=LAYER_VMEM),
        name="tail",
    )(z, factor, bias, gain, *front, weights, *firsts, *seconds)


def local(
    tokens,
    forget_offset,
    q_weight,
    k_weight,
    v_weight,
    forget_weight,
    forget_bias,
    score_gain,
    out_gain,
):
    x = tokens[0]
    rows, width = x.shape
    half = rows // 2
    heads = forget_bias.shape[0]
    dim = out_gain.shape[0] // heads
    n = lax.axis_size("sp")
    parts = lax.axis_size("dp")
    kv_heads = k_weight.shape[1] * parts // dim
    group = heads // kv_heads
    piece = 2 * k_weight.shape[1]
    z = lax.axis_index("sp").astype(jnp.int32).reshape(1)
    bf16, f32 = jnp.bfloat16, jnp.float32

    def padded(a):
        a = a.reshape(kv_heads, group, *a.shape[1:])
        return jnp.pad(a, ((0, 0), (0, PAD - group), (0, 0))).reshape(kv_heads * PAD, -1)

    gate_rows = kv_heads * PAD
    *sent, bias, weight_own = pl.pallas_call(
        pack_kernel,
        in_specs=[VM] * 7,
        out_specs=[VM] * 4,
        out_shape=[
            jax.ShapeDtypeStruct((half + PAD, width), bf16),
            jax.ShapeDtypeStruct((half, width), bf16),
            jax.ShapeDtypeStruct((gate_rows, rows), f32),
            jax.ShapeDtypeStruct((dim + piece, width), bf16),
        ],
        cost_estimate=pl.CostEstimate(
            flops=2 * rows * width * gate_rows, bytes_accessed=1 << 20, transcendentals=0
        ),
        compiler_params=pltpu.CompilerParams(vmem_limit_bytes=16 << 20),
        name="pack",
    )(
        x,
        padded(forget_weight.T),
        forget_offset,
        padded(forget_bias[:, None]),
        q_weight,
        k_weight.T,
        v_weight.T,
    )
    weight_all = lax.all_gather(weight_own, "dp", axis=0, tiled=False)

    sent, z, factor, bias, gain = lax.optimization_barrier(
        (
            sent,
            z,
            score_gain * (dim**-0.5 * LOG2_E),
            bias,
            out_gain[None, :],
        )
    )

    chains = [[block] + [None] * (n - 1) for block in sent]
    ups, downs = list(sent), list(sent)
    top = n - 1 - min(BACKS)
    late = [pair for pair in pairs_of(n) if pair[0] <= top < pair[0] + 2]
    early = [pair for pair in pairs_of(n) if pair not in late]
    for k in range(1, top + 1):
        rising = [(i, i + 1) for i in range(k - 1, n - 1)]
        for c, back in enumerate(BACKS):
            if k > n - 1 - back:
                continue
            if k <= back:
                sinking = [((b - k + 1) % n, (b - k) % n) for b in range(back)]
                down = lax.ppermute(downs[c], "sp", sinking)
            ups[c] = lax.ppermute(ups[c], "sp", rising)
            if k <= back:
                ups[c], downs[c] = lax.optimization_barrier((ups[c], down))
                chains[c][n - k] = downs[c]
            chains[c][k] = ups[c]

    front = front_call(z, weight_all, early, kv_heads, n, *chains)
    attended = tail_call(z, factor, bias, gain, front, weight_all, late, *chains)
    return attended[None]


def solution(mesh):
    in_specs = (
        P(("grp", "dp"), "sp", None),
        P(("grp", "dp"), "sp"),
        P(None, "dp"),
        P(None, "dp"),
        P(None, "dp"),
        P(),
        P(),
        P(),
        P(),
    )
    out_specs = P(("grp", "dp"), "sp", None)
    return jax.shard_map(local, mesh=mesh, in_specs=in_specs, out_specs=out_specs, check_vma=False)
```
